128 devices in a mesh: sp: 32 (over z, y, core), tp: 4 (over x).
Axes of the slice: x: 4, y: 4, z: 4, core: 2. Of those that a mesh axis runs over, the one named last changes fastest.
Arguments:
- tokens: bfloat16 [8192, 2048], P('sp'), may hold values from -6 to 6
- input_norm_gain: float32 [2048], replicated, may hold values from 0.1 to 1.9
- convolution_value_weight: bfloat16 [2048, 512], P(None, 'tp'), may hold values from -0.125 to 0.125
- convolution_gate_weight: bfloat16 [2048, 512], P(None, 'tp'), may hold values from -0.125 to 0.125
- depthwise_taps_weight: float32 [31, 512], P(None, 'tp'), may hold values from -1 to 1
- convolution_group_gain: float32 [512], P('tp'), may hold values from 0.1 to 1.9
- convolution_group_shift: float32 [512], P('tp'), may hold values from -3 to 3
- receptance_weight: bfloat16 [2048, 1024], P(None, 'tp'), may hold values from -0.125 to 0.125
- key_weight: bfloat16 [2048, 1024], P(None, 'tp'), may hold values from -0.125 to 0.125
- value_weight: bfloat16 [2048, 1024], P(None, 'tp'), may hold values from -0.125 to 0.125
- decay_weight: bfloat16 [2048, 1024], P(None, 'tp'), may hold values from -0.0625 to 0.0625
- correction_rate_weight: bfloat16 [2048, 1024], P(None, 'tp'), may hold values from -0.125 to 0.125
- output_gate_weight: bfloat16 [2048, 1024], P(None, 'tp'), may hold values from -0.125 to 0.125
- key_prenorm_gain: float32 [1024], P('tp'), may hold values from 0.04 to 8
- decay_offset_bias: float32 [1024], P('tp'), may hold values from -30 to 0
- position_decay_shift: float32 [8192, 1024], P('sp', 'tp'), may hold values from -1 to 1
- extra_log_decay: float32 [8192, 1024], P('sp', 'tp'), may hold values from -0.7 to 0
- head_norm_gain: float32 [1024], P('tp'), may hold values from 0.1 to 1.9
- convolution_output_weight: bfloat16 [512, 2048], replicated, may hold values from -0.15625 to 0.15625
- attention_output_weight: bfloat16 [1024, 2048], replicated, may hold values from -0.15625 to 0.15625
Outputs:
- mixed: bfloat16 [8192, 2048], P(('sp', 'tp'))
The draws below stay inside these ranges and needn't reach their ends.
All inputs are finite; a program needn't handle non-finite values.
Results may differ from the reference program's by a relative error of at most 0.0063.
The reference program's roundings to bfloat16 on the way (of `normed`, `conv_input`, `conv_out` and `mix_out`) count: a program that leaves them out, or rounds other values in their place, can miss the bound.
Values may be sent and summed in bfloat16 or wider, within the bound.
No kernel may reach another device: no remote copies, remote signals or barrier semaphores. Data moves between devices by JAX's collectives and lax.ppermute only.
A program may use at most 128 MiB of HBM per device.

```python
import jax
import jax.numpy as jnp
from jax import lax

D = 2048
CONV_CH = 512
CONV_TAPS = 31
HEADS = 16
HEAD = 64
TOKENS = 8192
MIX_CH = 1024


def draw_key_prenorm_gain(key, part):
    second = jax.random.fold_in(jax.random.fold_in(key, 53), 1)
    gain = jnp.exp(jnp.log(0.04) + jnp.log(200.0) * jax.random.uniform(second, (HEADS * HEAD,)))
    return jnp.clip(gain, 0.04, 8.0).astype(jnp.float32)


def draw_decay_offset_bias(key, part):
    first, second, third, fourth = jax.random.split(jax.random.fold_in(key, 11), 4)
    share = 0.5
    slow_head = jax.random.uniform(first, (HEADS,)) < share
    keep_scale = jnp.exp(jnp.log(0.1) + jnp.log(6.0) * jax.random.uniform(second, (HEADS,)))
    fast_length = jax.random.uniform(third, (HEADS,), minval=25.0, maxval=50.0)
    level = jnp.where(slow_head, jnp.log(keep_scale / TOKENS), -jnp.log(fast_length)) + 0.5
    jitter = jnp.clip(0.3 * jax.random.normal(fourth, (HEADS, HEAD)), -1.0, 1.0)
    return (level[:, None] + jitter).reshape(HEADS * HEAD).astype(jnp.float32)


def draw_position_decay_shift(key, part):
    level_key = jax.random.fold_in(key, 23)
    block_count = (TOKENS + 127) // 128
    level = jax.random.uniform(level_key, (block_count, HEADS), minval=-0.7, maxval=0.7)
    spread_rows = jnp.repeat(level, 128, axis=0)[:TOKENS]
    return jnp.repeat(spread_rows, HEAD, axis=1).astype(jnp.float32)


def draw_extra_log_decay(key, part):
    first, second = jax.random.split(jax.random.fold_in(key, 37), 2)
    places = jax.random.randint(first, (6,), 0, TOKENS)
    kept = jax.random.uniform(second, (6, HEADS * HEAD), minval=0.5, maxval=0.8)
    return jnp.zeros((TOKENS, HEADS * HEAD), jnp.float32).at[places].min(jnp.log(kept))


def level_of(stream_key, dims, pieces, smallest, top_value):
    def one(dim, shards_of):
        draws = jax.random.uniform(jax.random.fold_in(jax.random.fold_in(stream_key, 6), dim), (shards_of,), jnp.float32, smallest / len(pieces), top_value / len(pieces))
        return jnp.repeat(jnp.exp(draws), dims[dim] // shards_of).reshape((-1,) + (1,) * (len(dims) - dim - 1))

    factor_of = one(*pieces[0])
    for cut in pieces[1:]:
        factor_of = factor_of * one(*cut)
    return factor_of


def normal_values(rng, extent, spread, limit, cuts=(), kind=jnp.bfloat16):
    entries = spread * jax.random.normal(rng, extent, jnp.float32)
    if cuts:
        entries = entries * level_of(rng, extent, cuts, -0.22, 0.18)
    return jnp.clip(entries, -limit, limit).astype(kind)


def setup_inputs(seed: int = 0) -> dict:
    splits = jax.random.split(jax.random.key(seed), 21)
    tokens = normal_values(splits[0], (TOKENS, D), 1.0, 6.0, ((0, 32),))
    input_norm_gain = jnp.clip(1.0 + 0.18 * jax.random.normal(splits[1], (D,), jnp.float32), 0.1, 1.9)
    convolution_value_weight = normal_values(splits[2], (D, CONV_CH), D ** -0.5, 0.125, ((1, 4),))
    convolution_gate_weight = normal_values(splits[3], (D, CONV_CH), D ** -0.5, 0.125, ((1, 4),))
    depthwise_taps_weight = normal_values(splits[4], (CONV_TAPS, CONV_CH), CONV_TAPS ** -0.5, 1.0, ((1, 4),), jnp.float32)
    convolution_group_gain = jnp.clip(1.0 + 0.18 * jax.random.normal(splits[5], (CONV_CH,), jnp.float32), 0.1, 1.9)
    convolution_group_shift = normal_values(splits[6], (CONV_CH,), 0.5, 3.0, ((0, 4),), jnp.float32)
    receptance_weight = normal_values(splits[7], (D, MIX_CH), D ** -0.5, 0.125, ((1, 4),))
    key_weight = normal_values(splits[8], (D, MIX_CH), D ** -0.5, 0.125, ((1, 4),))
    value_weight = normal_values(splits[9], (D, MIX_CH), D ** -0.5, 0.125, ((1, 4),))
    decay_weight = normal_values(splits[10], (D, MIX_CH), (4 * D) ** -0.5, 0.0625, ((1, 4),))
    correction_rate_weight = normal_values(splits[11], (D, MIX_CH), D ** -0.5, 0.125, ((1, 4),))
    output_gate_weight = normal_values(splits[12], (D, MIX_CH), D ** -0.5, 0.125, ((1, 4),))
    key_prenorm_gain = draw_key_prenorm_gain(jax.random.fold_in(splits[20], 71), 0)
    decay_offset_bias = draw_decay_offset_bias(jax.random.fold_in(splits[20], 71), 0)
    position_decay_shift = draw_position_decay_shift(jax.random.fold_in(splits[20], 71), 0)
    extra_log_decay = draw_extra_log_decay(jax.random.fold_in(splits[20], 71), 0)
    head_norm_gain = jnp.clip(1.0 + 0.18 * jax.random.normal(splits[17], (MIX_CH,), jnp.float32), 0.1, 1.9)
    convolution_output_weight = normal_values(splits[18], (CONV_CH, D), (CONV_CH + MIX_CH) ** -0.5, 0.15625)
    attention_output_weight = normal_values(splits[19], (MIX_CH, D), (CONV_CH + MIX_CH) ** -0.5, 0.15625)
    return dict(tokens=tokens, input_norm_gain=input_norm_gain, convolution_value_weight=convolution_value_weight, convolution_gate_weight=convolution_gate_weight, depthwise_taps_weight=depthwise_taps_weight, convolution_group_gain=convolution_group_gain, convolution_group_shift=convolution_group_shift, receptance_weight=receptance_weight, key_weight=key_weight, value_weight=value_weight, decay_weight=decay_weight, correction_rate_weight=correction_rate_weight, output_gate_weight=output_gate_weight, key_prenorm_gain=key_prenorm_gain, decay_offset_bias=decay_offset_bias, position_decay_shift=position_decay_shift, extra_log_decay=extra_log_decay, head_norm_gain=head_norm_gain, convolution_output_weight=convolution_output_weight, attention_output_weight=attention_output_weight)


NORM_EPS = 1e-06
GROUP_EPS = 1e-05
HEAD_EPS = 0.00064
KEY_EPS = 1e-06

def stored(values):
    return lax.optimization_barrier(values.astype(jnp.bfloat16)).astype(jnp.float32)

def recurrence_step(state, inputs):
    receptance, decay, key_row, value_row, unit_key, erase_dir = inputs
    removed = jnp.einsum('hij,hj->hi', state, -unit_key)
    state = state * decay[:, None, :] + removed[:, :, None] * erase_dir[:, None, :] + value_row[:, :, None] * key_row[:, None, :]
    return (state, jnp.einsum('hij,hj->hi', state, receptance))

def reference(tokens, input_norm_gain, convolution_value_weight, convolution_gate_weight, depthwise_taps_weight, convolution_group_gain, convolution_group_shift, receptance_weight, key_weight, value_weight, decay_weight, correction_rate_weight, output_gate_weight, key_prenorm_gain, decay_offset_bias, position_decay_shift, extra_log_decay, head_norm_gain, convolution_output_weight, attention_output_weight):
    float_rows = tokens.astype(jnp.float32)
    normed = (float_rows * lax.rsqrt(lax.optimization_barrier(jnp.mean(float_rows * float_rows, axis=-1, keepdims=True)) + NORM_EPS) * input_norm_gain).astype(jnp.bfloat16)

    def project(weight):
        return stored(jnp.dot(normed, weight, preferred_element_type=jnp.float32))
    conv_input = stored(project(convolution_value_weight) * jax.nn.sigmoid(project(convolution_gate_weight)))
    padded = jnp.pad(conv_input, ((CONV_TAPS - 1, 0), (0, 0)))
    conv_sum = jnp.zeros((TOKENS, CONV_CH), jnp.float32)
    for offset in range(CONV_TAPS):
        conv_sum = conv_sum + depthwise_taps_weight[offset] * padded[offset:offset + TOKENS]
    grouped = conv_sum.reshape(TOKENS, CONV_CH // 64, 64)
    centred = grouped - lax.optimization_barrier(jnp.mean(grouped, axis=-1, keepdims=True))
    grouped = centred * lax.rsqrt(lax.optimization_barrier(jnp.mean(centred * centred, axis=-1, keepdims=True)) + GROUP_EPS)
    conv_out = jax.nn.silu(grouped.reshape(TOKENS, CONV_CH) * convolution_group_gain + convolution_group_shift).astype(jnp.bfloat16)
    receptance = project(receptance_weight)
    key_all = project(key_weight)
    value_all = project(value_weight)
    decay_logits = project(decay_weight) + decay_offset_bias + position_decay_shift
    decay_logarithm = -jnp.exp(-jax.nn.softplus(-decay_logits) - 0.5) + extra_log_decay
    erase_rate = jax.nn.sigmoid(project(correction_rate_weight))
    out_gate = jax.nn.sigmoid(project(output_gate_weight))

    def by_head(values):
        return values.reshape(TOKENS, HEADS, HEAD)
    unit_key = by_head(key_all * key_prenorm_gain)
    unit_key = unit_key * lax.rsqrt(lax.optimization_barrier(jnp.sum(unit_key * unit_key, axis=-1, keepdims=True)) + KEY_EPS)
    erase_dir = unit_key * by_head(erase_rate)
    start_state = jnp.zeros((HEADS, HEAD, HEAD), jnp.float32)
    _, readout = lax.scan(recurrence_step, start_state, (by_head(receptance), by_head(jnp.exp(decay_logarithm)), by_head(key_all), by_head(value_all), unit_key, erase_dir))
    centred_read = readout - lax.optimization_barrier(jnp.mean(readout, axis=-1, keepdims=True))
    normed_read = centred_read * lax.rsqrt(lax.optimization_barrier(jnp.mean(centred_read * centred_read, axis=-1, keepdims=True)) + HEAD_EPS)
    mix_out = (normed_read.reshape(TOKENS, HEADS * HEAD) * head_norm_gain * out_gate).astype(jnp.bfloat16)
    projected = jnp.dot(conv_out, convolution_output_weight, preferred_element_type=jnp.float32) + jnp.dot(mix_out, attention_output_weight, preferred_element_type=jnp.float32)
    return projected.astype(jnp.bfloat16)
```

```python
import jax
import jax.numpy as jnp
from jax import lax
from jax.experimental import pallas as pl
from jax.experimental.pallas import tpu as pltpu
from jax.sharding import Mesh
from jax.sharding import PartitionSpec as P

HEAD = 64
ROWS = 256
LANES = 256
CONV = 128
SPAN = 64
CHUNKS = ROWS // SPAN
HALO = 32
TAPS = 31
PACK = 2 * HEAD + HALO // 2
SP = ("z", "y", "c")
SP_TP = ("z", "y", "c", "x")

NORM_EPS = 1e-06
GROUP_EPS = 1e-05
HEAD_EPS = 0.00064
KEY_EPS = 1e-06
EXP_HALF = 0.6065306597126334

F32 = jnp.float32
BF16 = jnp.bfloat16
NN = (((1,), (0,)), ((), ()))
NT = (((1,), (1,)), ((), ()))
TN = (((0,), (0,)), ((), ()))
VMEM = pl.BlockSpec(memory_space=pltpu.VMEM)
ANY = pl.BlockSpec(memory_space=pl.ANY)


def mm(left, right, dims=NN):
    return lax.dot_general(
        left.astype(BF16), right.astype(BF16), dims, preferred_element_type=F32
    )


def halves(value):
    high = value.astype(BF16)
    return high, (value - high.astype(F32)).astype(BF16)


def mm3(left, right, dims=NN):
    left_high, left_low = halves(left)
    right_high, right_low = halves(right)
    return mm(left_high, right_high, dims) + (
        mm(left_high, right_low, dims) + mm(left_low, right_high, dims)
    )


def iota(shape, dim):
    return lax.broadcasted_iota(jnp.int32, shape, dim)


def head_lanes(shape, head):
    return (iota(shape, 1) // HEAD) == head


def block_ones(size):
    shape = (size, size)
    return jnp.where(iota(shape, 0) // HEAD == iota(shape, 1) // HEAD, 1.0, 0.0).astype(BF16)


def group_sum(value, ones):
    high, low = halves(value)
    return mm(high, ones) + mm(low, ones)


def expand(compact):
    shape = (LANES, LANES)
    tall = jnp.concatenate([compact] * (LANES // HEAD), axis=0)
    return jnp.where(iota(shape, 0) // HEAD == iota(shape, 1) // HEAD, tall, 0.0)


def shrink(full):
    parts = [full[HEAD * h : HEAD * (h + 1)] for h in range(LANES // HEAD)]
    return (parts[0] + parts[1]) + (parts[2] + parts[3])


def unit_state():
    shape = (HEAD, LANES)
    eye = jnp.where(iota(shape, 0) == iota(shape, 1) % HEAD, 1.0, 0.0)
    return jnp.concatenate([eye, jnp.zeros(shape, F32)], axis=0)


def follow(earlier, trans, base):
    moved = mm3(earlier, expand(trans))
    return jnp.concatenate([moved[:HEAD], moved[HEAD:] + base], axis=0)


def per_chunk(rows):
    return jnp.concatenate([jnp.broadcast_to(row, (SPAN, LANES)) for row in rows], axis=0)


def swap_pair(value):
    return pltpu.roll(value, HEAD, 1)


def local_kernel(
    tokens_hbm,
    gain,
    key_hbm,
    rate_hbm,
    decay_hbm,
    value_hbm,
    conv_value_hbm,
    conv_gate_hbm,
    receptance_hbm,
    gate_hbm,
    key_gain,
    bias,
    shift,
    extra,
    pack_out,
    prior_out,
    local_out,
    query_out,
    gate_out,
    conv_out,
    tokens,
    w_key,
    w_rate,
    w_decay,
    w_value,
    w_conv_value,
    w_conv_gate,
    w_receptance,
    w_gate,
    sems,
):
    pairs = (
        (tokens_hbm, tokens),
        (key_hbm, w_key),
        (rate_hbm, w_rate),
        (decay_hbm, w_decay),
        (value_hbm, w_value),
        (conv_value_hbm, w_conv_value),
        (conv_gate_hbm, w_conv_gate),
        (receptance_hbm, w_receptance),
        (gate_hbm, w_gate),
    )
    copies = [
        pltpu.make_async_copy(source, target, sems.at[n])
        for n, (source, target) in enumerate(pairs)
    ]
    for copy in copies:
        copy.start()
    copies[0].wait()
    rows = tokens[...].astype(F32)
    scale = lax.rsqrt(jnp.mean(rows * rows, axis=-1, keepdims=True) + NORM_EPS)
    normed = (rows * scale * gain[...]).astype(BF16)

    def project(n):
        copies[n].wait()
        return (
            jnp.dot(normed, pairs[n][1][...], preferred_element_type=F32)
            .astype(BF16)
            .astype(F32)
        )

    square = (ROWS, LANES)
    row_at, lane_at = iota(square, 0), iota(square, 1)
    same_chunk = row_at // SPAN == lane_at // SPAN
    ones = block_ones(LANES)

    key = project(1)
    key_scaled = key * key_gain[...]
    unit = key_scaled * lax.rsqrt(group_sum(key_scaled * key_scaled, ones) + KEY_EPS)
    erase = unit * jax.nn.sigmoid(project(2))
    logits = project(3) + bias[...] + shift[...]
    log_decay = extra[...] - EXP_HALF * jax.nn.sigmoid(logits)
    lower = jnp.where(same_chunk & (lane_at <= row_at), 1.0, 0.0).astype(BF16)
    part_high, rest = halves(log_decay)
    part_mid = rest
    part_low = (log_decay - part_high.astype(F32) - rest.astype(F32)).astype(BF16)
    cumulate = mm(lower, part_high) + (mm(lower, part_mid) + mm(lower, part_low))
    before = cumulate - log_decay
    mids = [cumulate[SPAN * c + 31 : SPAN * c + 32] for c in range(CHUNKS)]
    finals = [cumulate[SPAN * c + 63 : SPAN * c + 64] for c in range(CHUNKS)]
    mid = per_chunk(mids)
    rise = jnp.exp(mid - cumulate)
    fall_read = jnp.exp(cumulate - mid)
    unit_s = unit * jnp.exp(before - mid)
    erase_s = erase * rise
    key_s = key * rise
    from_start = per_chunk([jnp.exp(m) for m in mids])
    to_end = per_chunk([jnp.exp(f - m) for f, m in zip(finals, mids)])
    unit_q = unit_s * from_start
    kept_erase = (erase_s * to_end).astype(BF16)
    kept_key = (key_s * to_end).astype(BF16)
    erase_b = erase_s.astype(BF16)
    key_b = key_s.astype(BF16)
    value = project(4)
    value_b = value.astype(BF16)
    value_swapped = [swap_pair(value[:, :128]), swap_pair(value[:, 128:])]

    strict = same_chunk & (lane_at < row_at)
    near = strict & (row_at // 8 == lane_at // 8)
    far = strict & (row_at // 8 != lane_at // 8)
    low_half = iota((ROWS, 128), 1) < HEAD
    solved = []
    for h in range(4):
        pair, own = h // 2, (low_half if h % 2 == 0 else ~low_half)
        span = slice(128 * pair, 128 * pair + 128)
        left = jnp.where(head_lanes(square, h), unit_s, 0.0).astype(BF16)
        erase_mix = mm(left, erase_b, NT)
        key_mix = jnp.where(strict, mm(left, key_b, NT), 0.0)
        d1 = jnp.where(near, erase_mix, 0.0)
        n1 = jnp.where(far, erase_mix, 0.0)
        d2 = mm(d1, d1)
        d4 = mm(d2, d2)
        g = d2 - d1 - mm(d1, d2)
        dinv = g + d4 + mm(g, d4)
        p1 = n1 + mm(dinv, n1)
        p2 = mm(p1, p1)
        p4 = mm(p2, p2)
        key_value = mm(key_mix, value_swapped[pair])
        right = jnp.where(own, unit_q[:, span], key_value)
        y = right + mm(dinv, right)
        y = y + mm(p4, y)
        y = y + mm(p2, y)
        y = mm(p1, y) - y
        solved.append(y)
    weave = []
    removed = []
    for pair in range(2):
        even, odd = solved[2 * pair], solved[2 * pair + 1]
        weave.append(jnp.where(low_half, even, odd))
        removed.append(swap_pair(jnp.where(low_half, odd, even)))
    weave = jnp.concatenate(weave, axis=1).astype(BF16)
    removed = jnp.concatenate(removed, axis=1).astype(BF16)

    same_head = row_at // HEAD == lane_at // HEAD
    eye = row_at == lane_at
    state = unit_state()
    for c in range(CHUNKS):
        here = slice(SPAN * c, SPAN * c + SPAN)
        prior_out[c] = state
        full = mm(weave[here], kept_erase[here], TN)
        trans = jnp.where(same_head, full, 0.0) + jnp.where(
            eye, jnp.broadcast_to(jnp.exp(finals[c]), square), 0.0
        )
        base = mm(removed[here], kept_erase[here], TN) + mm(value_b[here], kept_key[here], TN)
        base = shrink(jnp.where(same_head, base, 0.0))
        moved = mm3(state, trans)
        state = jnp.concatenate([moved[:HEAD], moved[HEAD:] + base], axis=0)
    pack_out[: 2 * HEAD] = state

    conv_input = (project(5) * jax.nn.sigmoid(project(6))).astype(BF16).astype(F32)
    conv_out[...] = conv_input
    pack_out[2 * HEAD :, :128] = conv_input[ROWS - 32 : ROWS - 16]
    pack_out[2 * HEAD :, 128:] = conv_input[ROWS - 16 :]

    receptance = project(7)
    gate_out[...] = jax.nn.sigmoid(project(8))
    read_s = receptance * fall_read
    read_q = read_s * from_start
    inclusive = same_chunk & (lane_at <= row_at)
    found = []
    for h in range(4):
        pair, own = h // 2, (low_half if h % 2 == 0 else ~low_half)
        left = jnp.where(head_lanes(square, h), read_s, 0.0).astype(BF16)
        read_erase = jnp.where(inclusive, mm(left, erase_b, NT), 0.0)
        read_key = jnp.where(inclusive, mm(left, key_b, NT), 0.0)
        mine = jnp.where(own, 0.0, value_swapped[pair])
        found.append(mm(read_erase, solved[h]) + mm(read_key, mine))
    query, local = [], []
    for pair in range(2):
        even, odd = found[2 * pair], found[2 * pair + 1]
        query.append(jnp.where(low_half, even, odd))
        local.append(swap_pair(jnp.where(low_half, odd, even)))
    query = jnp.concatenate(query, axis=1) + read_q
    local = jnp.concatenate(local, axis=1)
    for c in range(CHUNKS):
        here = slice(SPAN * c, SPAN * c + SPAN)
        if c == 0:
            local_out[here] = local[here]
            query_out[here] = query[here].astype(BF16)
        else:
            prior = prior_out[c]
            local_out[here] = local[here] + mm(query[here], expand(prior[HEAD:]), NT)
            query_out[here] = mm(query[here], expand(prior[:HEAD]), NT).astype(BF16)


def conv_kernel(conv_in, taps, gain, shift, done_out, part_out, padded):
    padded[:HALO] = jnp.zeros((HALO, CONV), F32)
    padded[HALO:] = conv_in[...]
    total = jnp.zeros((ROWS, CONV), F32)
    for j in range(TAPS):
        total = total + taps[j : j + 1] * padded[2 + j : 2 + j + ROWS]
    part_out[...] = total[:HALO]
    done_out[...] = finish_conv(total, gain[...], shift[...])


def finish_conv(total, gain, shift):
    ones = block_ones(CONV)
    centred = total - group_sum(total, ones) * (1.0 / HEAD)
    spread = group_sum(centred * centred, ones) * (1.0 / HEAD)
    scaled = centred * lax.rsqrt(spread + GROUP_EPS) * gain + shift
    return (scaled * jax.nn.sigmoid(scaled)).astype(BF16)


def core_kernel(mine, other, pack_out, prefix_out):
    first = lax.axis_index("c") == 0
    early = jnp.where(first, mine[...], other[...])
    late = jnp.where(first, other[...], mine[...])
    joined = follow(early[: 2 * HEAD], late[:HEAD], late[HEAD : 2 * HEAD])
    pack_out[: 2 * HEAD] = joined.astype(BF16)
    pack_out[2 * HEAD :] = late[2 * HEAD :].astype(BF16)
    prefix_out[...] = jnp.where(first, unit_state(), early[: 2 * HEAD])


def row_kernel(own, from_1, from_2, from_3, prefix, pack_out, prefix_out, slots):
    me = lax.axis_index("y")
    for n, ref in enumerate((own, from_1, from_2, from_3)):
        slots[n] = ref[...].astype(F32)
    state = unit_state()
    before = state
    for n in range(4):
        before = jnp.where(me == n, state, before)
        piece = slots[lax.rem(me - n + 4, 4)]
        if n == 0:
            state = piece[: 2 * HEAD]
        else:
            state = follow(state, piece[:HEAD], piece[HEAD : 2 * HEAD])
        if n == 3:
            pack_out[2 * HEAD :] = piece[2 * HEAD :].astype(BF16)
    pack_out[: 2 * HEAD] = state.astype(BF16)
    prefix_out[...] = follow(before, prefix[:HEAD], prefix[HEAD:])


def last_kernel(
    from_1,
    from_2,
    from_3,
    prefix,
    side_core,
    side_row,
    local,
    query,
    gate,
    head_gain,
    conv_done,
    conv_part,
    taps,
    conv_gain,
    conv_shift,
    out_0,
    out_1,
    out_2,
    out_3,
    slots,
    ready,
    padded,
):
    z, y, c, x = (lax.axis_index(name) for name in SP_TP)
    for n, ref in enumerate((from_1, from_2, from_3)):
        slots[n] = ref[: 2 * HEAD].astype(F32)
    state = jnp.zeros((HEAD, LANES), F32)
    for n in range(3):
        piece = slots[lax.rem(z - n + 3, 4)] if n else slots[jnp.maximum(z - 1, 0)]
        if n:
            piece = slots[jnp.clip(z - n - 1, 0, 2)]
            moved = mm3(state, expand(piece[:HEAD])) + piece[HEAD:]
        else:
            moved = piece[HEAD:]
        state = jnp.where(n < z, moved, state)
    state = mm3(state, expand(prefix[:HEAD])) + prefix[HEAD:]
    readout = local[...] + mm(query[...], expand(state), NT)
    ones = block_ones(LANES)
    centred = readout - group_sum(readout, ones) * (1.0 / HEAD)
    spread = group_sum(centred * centred, ones) * (1.0 / HEAD)
    mixed = centred * lax.rsqrt(spread + HEAD_EPS) * head_gain[...] * gate[...]
    ready[:, CONV:] = mixed.astype(BF16)
    ready[:, :CONV] = conv_done[...]

    far = jnp.where(y > 0, side_row[2 * HEAD :].astype(F32), from_1[2 * HEAD :].astype(F32))
    far = jnp.where((y == 0) & (z == 0), 0.0, far)
    side = jnp.where(c == 1, side_core[2 * HEAD :], far)
    padded[:16] = side[:, :128]
    padded[16:32] = side[:, 128:]
    padded[32:] = jnp.zeros((HALO, CONV), F32)
    total = conv_part[...]
    for j in range(TAPS):
        total = total + taps[j : j + 1] * padded[2 + j : 2 + j + HALO]
    ready[:HALO, :CONV] = finish_conv(total, conv_gain[...], conv_shift[...])
    for n, out in enumerate((out_0, out_1, out_2, out_3)):
        to = lax.rem(x + n, 4)
        out[...] = ready[pl.ds(pl.multiple_of(to * SPAN, SPAN), SPAN)]


def project_kernel(own, from_1, from_2, from_3, conv_hbm, mix_hbm, out, conv_w, mix_w, sems):
    x = lax.axis_index("x")
    copies = [
        pltpu.make_async_copy(conv_hbm, conv_w, sems.at[0]),
        pltpu.make_async_copy(mix_hbm, mix_w, sems.at[1]),
    ]
    for copy in copies:
        copy.start()
    for copy in copies:
        copy.wait()
    total = jnp.zeros((SPAN, 2048), F32)
    for n, ref in enumerate((own, from_1, from_2, from_3)):
        of = lax.rem(x - n + 4, 4)
        total = total + jnp.dot(
            ref[:, :CONV],
            conv_w[pl.ds(pl.multiple_of(of * CONV, CONV), CONV)],
            preferred_element_type=F32,
        )
        total = total + jnp.dot(
            ref[:, CONV:],
            mix_w[pl.ds(pl.multiple_of(of * LANES, LANES), LANES)],
            preferred_element_type=F32,
        )
    out[...] = total.astype(BF16)


def shifted(value, axis, steps):
    count = lax.axis_size(axis)
    return lax.ppermute(value, axis, [(s, (s + steps) % count) for s in range(count)])


def params():
    return pltpu.CompilerParams(vmem_limit_bytes=40 * 1024 * 1024)


def call(kernel, name, outs, arguments, specs=None, scratch=()):
    return pl.pallas_call(
        kernel,
        name=name,
        out_shape=[jax.ShapeDtypeStruct(*o) for o in outs],
        in_specs=specs or [VMEM] * len(arguments),
        out_specs=[VMEM] * len(outs),
        scratch_shapes=list(scratch),
        compiler_params=params(),
    )(*arguments)


def local(
    tokens,
    input_norm_gain,
    convolution_value_weight,
    convolution_gate_weight,
    depthwise_taps_weight,
    convolution_group_gain,
    convolution_group_shift,
    receptance_weight,
    key_weight,
    value_weight,
    decay_weight,
    correction_rate_weight,
    output_gate_weight,
    key_prenorm_gain,
    decay_offset_bias,
    position_decay_shift,
    extra_log_decay,
    head_norm_gain,
    convolution_output_weight,
    attention_output_weight,
):
    def as_row(value):
        return value.reshape(1, value.shape[0])

    conv_gain, conv_shift = as_row(convolution_group_gain), as_row(convolution_group_shift)
    wide = (2048, LANES)
    thin = (2048, CONV)
    pack, _, local_read, query, gate, conv_input = call(
        local_kernel,
        "local",
        [
            ((PACK, LANES), F32),
            ((CHUNKS, 2 * HEAD, LANES), F32),
            ((ROWS, LANES), F32),
            ((ROWS, LANES), BF16),
            ((ROWS, LANES), F32),
            ((ROWS, CONV), F32),
        ],
        (
            tokens,
            as_row(input_norm_gain),
            key_weight,
            correction_rate_weight,
            decay_weight,
            value_weight,
            convolution_value_weight,
            convolution_gate_weight,
            receptance_weight,
            output_gate_weight,
            as_row(key_prenorm_gain),
            as_row(decay_offset_bias),
            position_decay_shift,
            extra_log_decay,
        ),
        specs=[ANY, VMEM] + [ANY] * 8 + [VMEM] * 4,
        scratch=[pltpu.VMEM((ROWS, 2048), BF16)]
        + [pltpu.VMEM(wide, BF16)] * 4
        + [pltpu.VMEM(thin, BF16)] * 2
        + [pltpu.VMEM(wide, BF16)] * 2
        + [pltpu.SemaphoreType.DMA((9,))],
    )
    other = shifted(pack, "c", 1)
    conv_done, conv_part = call(
        conv_kernel,
        "conv",
        [((ROWS, CONV), BF16), ((HALO, CONV), F32)],
        (conv_input, depthwise_taps_weight, conv_gain, conv_shift),
        scratch=[pltpu.VMEM((HALO + ROWS, CONV), F32)],
    )
    pack_y, prefix_c = call(
        core_kernel,
        "core",
        [((PACK, LANES), BF16), ((2 * HEAD, LANES), F32)],
        (pack, other),
    )
    rows = [shifted(pack_y, "y", n) for n in (1, 2, 3)]
    pack_z, prefix = call(
        row_kernel,
        "row",
        [((PACK, LANES), BF16), ((2 * HEAD, LANES), F32)],
        (pack_y, *rows, prefix_c),
        scratch=[pltpu.VMEM((4, PACK, LANES), F32)],
    )
    planes = [shifted(pack_z, "z", n) for n in (1, 2, 3)]
    sends = call(
        last_kernel,
        "last",
        [((SPAN, CONV + LANES), BF16)] * 4,
        (
            *planes,
            prefix,
            other,
            rows[0],
            local_read,
            query,
            gate,
            as_row(head_norm_gain),
            conv_done,
            conv_part,
            depthwise_taps_weight,
            conv_gain,
            conv_shift,
        ),
        scratch=[
            pltpu.VMEM((3, 2 * HEAD, LANES), F32),
            pltpu.VMEM((ROWS, CONV + LANES), BF16),
            pltpu.VMEM((2 * HALO, CONV), F32),
        ],
    )
    arrived = [shifted(sends[n], "x", n) for n in (1, 2, 3)]
    (mixed,) = call(
        project_kernel,
        "project",
        [((SPAN, 2048), BF16)],
        (sends[0], *arrived, convolution_output_weight, attention_output_weight),
        specs=[VMEM] * 4 + [ANY] * 2,
        scratch=[
            pltpu.VMEM((512, 2048), BF16),
            pltpu.VMEM((1024, 2048), BF16),
            pltpu.SemaphoreType.DMA((2,)),
        ],
    )
    return mixed


def solution(mesh):
    split = Mesh(mesh.devices.reshape(4, 4, 2, mesh.shape["tp"]), SP_TP)
    placed = (
        P(SP, None),
        P(),
        P(None, "x"),
        P(None, "x"),
        P(None, "x"),
        P("x"),
        P("x"),
        P(None, "x"),
        P(None, "x"),
        P(None, "x"),
        P(None, "x"),
        P(None, "x"),
        P(None, "x"),
        P("x"),
        P("x"),
        P(SP, "x"),
        P(SP, "x"),
        P("x"),
        P(),
        P(),
    )
    return jax.shard_map(
        local, mesh=split, in_specs=placed, out_specs=P(SP_TP, None), check_vma=False
    )
```

```python
import functools

import jax
import jax.numpy as jnp
from jax import lax
from jax.experimental import pallas as pl
from jax.experimental.pallas import tpu as pltpu
from jax.sharding import Mesh
from jax.sharding import PartitionSpec as P

HEAD = 64
ROWS = 256
LANES = 256
CONV = 128
SPAN = 64
CHUNKS = ROWS // SPAN
HALO = 32
TAPS = 31
PACK = 2 * HEAD + HALO // 2
SP = ("z", "y", "c")
SP_TP = ("z", "y", "c", "x")

NORM_EPS = 1e-06
GROUP_EPS = 1e-05
HEAD_EPS = 0.00064
KEY_EPS = 1e-06
EXP_HALF = 0.6065306597126334

F32 = jnp.float32
BF16 = jnp.bfloat16
NN = (((1,), (0,)), ((), ()))
NT = (((1,), (1,)), ((), ()))
TN = (((0,), (0,)), ((), ()))
VMEM = pl.BlockSpec(memory_space=pltpu.VMEM)
HBM = pl.BlockSpec(memory_space=pltpu.HBM)


def mm(left, right, dims=NN):
    return lax.dot_general(
        left.astype(BF16), right.astype(BF16), dims, preferred_element_type=F32
    )


def halves(value):
    high = value.astype(BF16)
    return high, (value - high.astype(F32)).astype(BF16)


def mm3(left, right, dims=NN):
    left_high, left_low = halves(left)
    right_high, right_low = halves(right)
    return mm(left_high, right_high, dims) + (
        mm(left_high, right_low, dims) + mm(left_low, right_high, dims)
    )


def iota(shape, dim):
    return lax.broadcasted_iota(jnp.int32, shape, dim)


def head_lanes(shape, head):
    return (iota(shape, 1) // HEAD) == head


def block_ones(size):
    shape = (size, size)
    return jnp.where(iota(shape, 0) // HEAD == iota(shape, 1) // HEAD, 1.0, 0.0).astype(BF16)


def group_sum(value, ones):
    high, low = halves(value)
    return mm(high, ones) + mm(low, ones)


def expand(compact):
    shape = (LANES, LANES)
    tall = jnp.concatenate([compact] * (LANES // HEAD), axis=0)
    return jnp.where(iota(shape, 0) // HEAD == iota(shape, 1) // HEAD, tall, 0.0)


def shrink(full):
    parts = [full[HEAD * h : HEAD * (h + 1)] for h in range(LANES // HEAD)]
    return (parts[0] + parts[1]) + (parts[2] + parts[3])


def unit_state():
    shape = (HEAD, LANES)
    eye = jnp.where(iota(shape, 0) == iota(shape, 1) % HEAD, 1.0, 0.0)
    return jnp.concatenate([eye, jnp.zeros(shape, F32)], axis=0)


def follow(earlier, trans, base):
    moved = mm3(earlier, expand(trans))
    return jnp.concatenate([moved[:HEAD], moved[HEAD:] + base], axis=0)


def per_chunk(rows):
    return jnp.concatenate([jnp.broadcast_to(row, (SPAN, LANES)) for row in rows], axis=0)


def swap_pair(value):
    return pltpu.roll(value, HEAD, 1)


def local_kernel(*refs):
    sources = refs[:12]
    pack_out, prior_out, conv_out, normed_out, fall_out, start_out = refs[12:18]
    erase_out, key_out, value_out, solved_out = refs[18:22]
    targets = refs[22:34]
    sems = refs[34]
    copies = [
        pltpu.make_async_copy(source, target, sems.at[n])
        for n, (source, target) in enumerate(zip(sources, targets))
    ]
    for copy in copies:
        copy.start()
    tokens, gain, key_gain, bias, shift, extra = targets[:6]
    copies[0].wait()
    copies[1].wait()
    rows = tokens[...].astype(F32)
    scale = lax.rsqrt(jnp.mean(rows * rows, axis=-1, keepdims=True) + NORM_EPS)
    normed = (rows * scale * gain[...]).astype(BF16)
    normed_out[...] = normed

    def project(n):
        copies[n].wait()
        return rounded_product(normed, targets[n][...])

    square = (ROWS, LANES)
    row_at, lane_at = iota(square, 0), iota(square, 1)
    same_chunk = row_at // SPAN == lane_at // SPAN
    ones = block_ones(LANES)

    key = project(6)
    copies[2].wait()
    key_scaled = key * key_gain[...]
    unit = key_scaled * lax.rsqrt(group_sum(key_scaled * key_scaled, ones) + KEY_EPS)
    erase = unit * jax.nn.sigmoid(project(7))
    decay = project(8)
    for n in (3, 4, 5):
        copies[n].wait()
    logits = decay + bias[...] + shift[...]
    log_decay = extra[...] - EXP_HALF * jax.nn.sigmoid(logits)
    lower = jnp.where(same_chunk & (lane_at <= row_at), 1.0, 0.0).astype(BF16)
    part_high, part_mid = halves(log_decay)
    part_low = (log_decay - part_high.astype(F32) - part_mid.astype(F32)).astype(BF16)
    cumulate = mm(lower, part_high) + (mm(lower, part_mid) + mm(lower, part_low))
    before = cumulate - log_decay
    mids = [cumulate[SPAN * c + 31 : SPAN * c + 32] for c in range(CHUNKS)]
    finals = [cumulate[SPAN * c + 63 : SPAN * c + 64] for c in range(CHUNKS)]
    mid = per_chunk(mids)
    rise = jnp.exp(mid - cumulate)
    fall_out[...] = jnp.exp(cumulate - mid)
    unit_s = unit * jnp.exp(before - mid)
    erase_s = erase * rise
    key_s = key * rise
    starts = [jnp.exp(m) for m in mids]
    for c in range(CHUNKS):
        start_out[c : c + 1] = starts[c]
    to_end = per_chunk([jnp.exp(f - m) for f, m in zip(finals, mids)])
    unit_q = unit_s * per_chunk(starts)
    kept_erase = (erase_s * to_end).astype(BF16)
    kept_key = (key_s * to_end).astype(BF16)
    erase_b = erase_s.astype(BF16)
    key_b = key_s.astype(BF16)
    value = project(9)
    value_b = value.astype(BF16)
    value_swapped = [
        swap_pair(value[:, :128]).astype(BF16),
        swap_pair(value[:, 128:]).astype(BF16),
    ]
    erase_out[...] = erase_b
    key_out[...] = key_b
    value_out[:, :128] = value_swapped[0]
    value_out[:, 128:] = value_swapped[1]

    strict = same_chunk & (lane_at < row_at)
    near = strict & (row_at // 8 == lane_at // 8)
    far = strict & (row_at // 8 != lane_at // 8)
    low_half = iota((ROWS, 128), 1) < HEAD
    solved = []
    for h in range(4):
        pair, own = h // 2, (low_half if h % 2 == 0 else ~low_half)
        span = slice(128 * pair, 128 * pair + 128)
        left = jnp.where(head_lanes(square, h), unit_s, 0.0).astype(BF16)
        erase_mix = mm(left, erase_b, NT)
        key_mix = jnp.where(strict, mm(left, key_b, NT), 0.0)
        d1 = jnp.where(near, erase_mix, 0.0)
        n1 = jnp.where(far, erase_mix, 0.0)
        d2 = mm(d1, d1)
        d4 = mm(d2, d2)
        g = d2 - d1 - mm(d1, d2)
        dinv = g + d4 + mm(g, d4)
        p1 = n1 + mm(dinv, n1)
        p2 = mm(p1, p1)
        p4 = mm(p2, p2)
        key_value = mm(key_mix, value_swapped[pair])
        right = jnp.where(own, unit_q[:, span], key_value)
        y = right + mm(dinv, right)
        y = y + mm(p4, y)
        y = y + mm(p2, y)
        y = mm(p1, y) - y
        solved.append(y)
        solved_out[h] = y.astype(BF16)
    weave = []
    removed = []
    for pair in range(2):
        even, odd = solved[2 * pair], solved[2 * pair + 1]
        weave.append(jnp.where(low_half, even, odd))
        removed.append(swap_pair(jnp.where(low_half, odd, even)))
    weave = jnp.concatenate(weave, axis=1).astype(BF16)
    removed = jnp.concatenate(removed, axis=1).astype(BF16)

    same_head = row_at // HEAD == lane_at // HEAD
    eye = row_at == lane_at
    state = unit_state()
    for c in range(CHUNKS):
        here = slice(SPAN * c, SPAN * c + SPAN)
        prior_out[c] = state
        full = mm(weave[here], kept_erase[here], TN)
        trans = jnp.where(same_head, full, 0.0) + jnp.where(
            eye, jnp.broadcast_to(jnp.exp(finals[c]), square), 0.0
        )
        base = mm(removed[here], kept_erase[here], TN) + mm(value_b[here], kept_key[here], TN)
        base = shrink(jnp.where(same_head, base, 0.0))
        moved = mm3(state, trans)
        state = jnp.concatenate([moved[:HEAD], moved[HEAD:] + base], axis=0)
    pack_out[: 2 * HEAD] = state

    conv_input = rounded(project(10) * jax.nn.sigmoid(project(11)))
    conv_out[...] = conv_input
    pack_out[2 * HEAD :, :128] = conv_input[ROWS - 32 : ROWS - 16]
    pack_out[2 * HEAD :, 128:] = conv_input[ROWS - 16 :]


def rounded(value):
    return value.astype(BF16).astype(F32)


def rounded_product(left, right):
    return rounded(jnp.dot(left, right, preferred_element_type=F32))


def read_kernel(
    normed,
    w_receptance,
    w_gate,
    fall,
    start,
    erase,
    key,
    value_swapped,
    solved,
    priors,
    local_out,
    query_out,
    gate_out,
):
    square = (ROWS, LANES)
    row_at, lane_at = iota(square, 0), iota(square, 1)
    low_half = iota((ROWS, 128), 1) < HEAD
    receptance = rounded_product(normed[...], w_receptance[...])
    gate_out[...] = jax.nn.sigmoid(rounded_product(normed[...], w_gate[...]))
    read_s = receptance * fall[...]
    read_q = read_s * per_chunk([start[c : c + 1] for c in range(CHUNKS)])
    inclusive = (row_at // SPAN == lane_at // SPAN) & (lane_at <= row_at)
    found = []
    for h in range(4):
        pair, own = h // 2, (low_half if h % 2 == 0 else ~low_half)
        span = slice(128 * pair, 128 * pair + 128)
        left = jnp.where(head_lanes(square, h), read_s, 0.0).astype(BF16)
        read_erase = jnp.where(inclusive, mm(left, erase[...], NT), 0.0)
        read_key = jnp.where(inclusive, mm(left, key[...], NT), 0.0)
        mine = jnp.where(own, 0.0, value_swapped[:, span].astype(F32))
        found.append(mm(read_erase, solved[h]) + mm(read_key, mine))
    query, local = [], []
    for pair in range(2):
        even, odd = found[2 * pair], found[2 * pair + 1]
        query.append(jnp.where(low_half, even, odd))
        local.append(swap_pair(jnp.where(low_half, odd, even)))
    query = jnp.concatenate(query, axis=1) + read_q
    local = jnp.concatenate(local, axis=1)
    for c in range(CHUNKS):
        here = slice(SPAN * c, SPAN * c + SPAN)
        if c == 0:
            local_out[here] = local[here]
            query_out[here] = query[here].astype(BF16)
        else:
            prior = priors[c]
            local_out[here] = local[here] + mm(query[here], expand(prior[HEAD:]), NT)
            query_out[here] = mm(query[here], expand(prior[:HEAD]), NT).astype(BF16)


def conv_kernel(conv_in, taps, gain, shift, done_out, part_out, padded):
    padded[:HALO] = jnp.zeros((HALO, CONV), F32)
    padded[HALO:] = conv_in[...]
    total = jnp.zeros((ROWS, CONV), F32)
    for j in range(TAPS):
        total = total + taps[j : j + 1] * padded[2 + j : 2 + j + ROWS]
    part_out[...] = total[:HALO]
    done_out[...] = finish_conv(total, gain[...], shift[...])


def finish_conv(total, gain, shift):
    ones = block_ones(CONV)
    centred = total - group_sum(total, ones) * (1.0 / HEAD)
    spread = group_sum(centred * centred, ones) * (1.0 / HEAD)
    scaled = centred * lax.rsqrt(spread + GROUP_EPS) * gain + shift
    return (scaled * jax.nn.sigmoid(scaled)).astype(BF16)


def joined(lower, upper):
    return follow(lower[: 2 * HEAD], upper[:HEAD], upper[HEAD : 2 * HEAD])


def core_kernel(mine, other, pack_out, total_out, prefix_out):
    first = lax.axis_index("c") == 0
    early = jnp.where(first, mine[...], other[...])
    late = jnp.where(first, other[...], mine[...])
    total = joined(early, late)
    total_out[...] = total
    pack_out[: 2 * HEAD] = total.astype(BF16)
    pack_out[2 * HEAD :] = late[2 * HEAD :].astype(BF16)
    prefix_out[: 2 * HEAD] = jnp.where(first, unit_state(), early[: 2 * HEAD])
    prefix_out[2 * HEAD :] = jnp.where(first, 0.0, early[2 * HEAD :])


def pair_kernel(axis, far, sent, mine, total, other, prefix, pack_out, total_out, prefix_out):
    at = lax.axis_index(axis)
    upper = (at >= 2) if far else (lax.rem(at, 2) == 1)
    got = other[...].astype(F32)
    states = got[: 2 * HEAD]
    early = jnp.where(upper, states, total[...])
    late = jnp.where(upper, total[...], states)
    result = joined(early, late)
    total_out[...] = result
    pack_out[: HEAD * sent] = result[HEAD * (2 - sent) :].astype(BF16)
    tail = other if far else mine
    pack_out[HEAD * sent :] = tail[2 * HEAD :]
    behind = joined(states, prefix[...])
    prefix_out[: 2 * HEAD] = jnp.where(upper, behind, prefix[: 2 * HEAD])
    takes = (at == 2) if far else upper
    takes = takes & (lax.axis_index("c") == 0)
    if axis == "z":
        takes = takes & (lax.axis_index("y") == 0)
    prefix_out[2 * HEAD :] = jnp.where(takes, got[2 * HEAD :], prefix[2 * HEAD :])


def last_kernel(
    other,
    prefix,
    local,
    query,
    gate,
    head_gain,
    conv_done,
    conv_part,
    taps,
    conv_gain,
    conv_shift,
    out_0,
    out_1,
    out_2,
    out_3,
    ready,
    padded,
):
    z, y, c, x = (lax.axis_index(name) for name in SP_TP)
    got = other[...].astype(F32)
    entering = jnp.where(z >= 2, got[:HEAD], 0.0)
    state = mm3(entering, expand(prefix[:HEAD])) + prefix[HEAD : 2 * HEAD]
    readout = local[...] + mm(query[...], expand(state), NT)
    ones = block_ones(LANES)
    centred = readout - group_sum(readout, ones) * (1.0 / HEAD)
    spread = group_sum(centred * centred, ones) * (1.0 / HEAD)
    mixed = centred * lax.rsqrt(spread + HEAD_EPS) * head_gain[...] * gate[...]
    ready[:, CONV:] = mixed.astype(BF16)
    ready[:, :CONV] = conv_done[...]

    takes = (z == 2) & (y == 0) & (c == 0)
    side = jnp.where(takes, got[HEAD:], prefix[2 * HEAD :])
    padded[:16] = side[:, :128]
    padded[16:32] = side[:, 128:]
    padded[32:] = jnp.zeros((HALO, CONV), F32)
    total = conv_part[...]
    for j in range(TAPS):
        total = total + taps[j : j + 1] * padded[2 + j : 2 + j + HALO]
    ready[:HALO, :CONV] = finish_conv(total, conv_gain[...], conv_shift[...])
    for n, out in enumerate((out_0, out_1, out_2, out_3)):
        to = lax.rem(x + n, 4)
        out[...] = ready[pl.ds(pl.multiple_of(to * SPAN, SPAN), SPAN)]


def project_kernel(own, from_1, from_2, from_3, conv_w, mix_w, out):
    x = lax.axis_index("x")
    total = jnp.zeros((SPAN, 2048), F32)
    for n, ref in enumerate((own, from_1, from_2, from_3)):
        of = lax.rem(x - n + 4, 4)
        total = total + jnp.dot(
            ref[:, :CONV],
            conv_w[pl.ds(pl.multiple_of(of * CONV, CONV), CONV)],
            preferred_element_type=F32,
        )
        total = total + jnp.dot(
            ref[:, CONV:],
            mix_w[pl.ds(pl.multiple_of(of * LANES, LANES), LANES)],
            preferred_element_type=F32,
        )
    out[...] = total.astype(BF16)


def shifted(value, axis, steps):
    count = lax.axis_size(axis)
    return lax.ppermute(value, axis, [(s, (s + steps) % count) for s in range(count)])


def swapped(value, axis, bits):
    count = lax.axis_size(axis)
    return lax.ppermute(value, axis, [(s, s ^ bits) for s in range(count)])


def params():
    return pltpu.CompilerParams(vmem_limit_bytes=40 * 1024 * 1024)


def call(kernel, name, outs, arguments, specs=None, scratch=()):
    return pl.pallas_call(
        kernel,
        name=name,
        out_shape=[jax.ShapeDtypeStruct(*o) for o in outs],
        in_specs=specs or [VMEM] * len(arguments),
        out_specs=[VMEM] * len(outs),
        scratch_shapes=list(scratch),
        compiler_params=params(),
    )(*arguments)


def local(
    tokens,
    input_norm_gain,
    convolution_value_weight,
    convolution_gate_weight,
    depthwise_taps_weight,
    convolution_group_gain,
    convolution_group_shift,
    receptance_weight,
    key_weight,
    value_weight,
    decay_weight,
    correction_rate_weight,
    output_gate_weight,
    key_prenorm_gain,
    decay_offset_bias,
    position_decay_shift,
    extra_log_decay,
    head_norm_gain,
    convolution_output_weight,
    attention_output_weight,
):
    def as_row(value):
        return value.reshape(1, value.shape[0])

    conv_gain, conv_shift = as_row(convolution_group_gain), as_row(convolution_group_shift)
    wide = pltpu.VMEM((2048, LANES), BF16)
    thin = pltpu.VMEM((2048, CONV), BF16)
    row = pltpu.VMEM((1, LANES), F32)
    square = ((ROWS, LANES), F32)
    square_b = ((ROWS, LANES), BF16)
    state = ((2 * HEAD, LANES), F32)
    packed = ((PACK, LANES), F32)
    packed_b = ((PACK, LANES), BF16)
    pack, priors, conv_input, normed, fall, start, erase, key, value_swapped, solved = call(
        local_kernel,
        "local",
        [
            packed,
            ((CHUNKS, 2 * HEAD, LANES), F32),
            ((ROWS, CONV), F32),
            ((ROWS, 2048), BF16),
            square,
            ((8, LANES), F32),
            square_b,
            square_b,
            square_b,
            ((4, ROWS, CONV), BF16),
        ],
        (
            tokens,
            as_row(input_norm_gain),
            as_row(key_prenorm_gain),
            as_row(decay_offset_bias),
            position_decay_shift,
            extra_log_decay,
            key_weight,
            correction_rate_weight,
            decay_weight,
            value_weight,
            convolution_value_weight,
            convolution_gate_weight,
        ),
        specs=[HBM] * 12,
        scratch=[pltpu.VMEM((ROWS, 2048), BF16), pltpu.VMEM((1, 2048), F32), row, row]
        + [pltpu.VMEM((ROWS, LANES), F32)] * 2
        + [wide] * 4
        + [thin] * 2
        + [pltpu.SemaphoreType.DMA((12,))],
    )
    other = swapped(pack, "c", 1)
    pack, total, prefix = call(core_kernel, "core", [packed_b, state, packed], (pack, other))
    local_read, query, gate = call(
        read_kernel,
        "read",
        [square, square_b, square],
        (
            normed,
            receptance_weight,
            output_gate_weight,
            fall,
            start,
            erase,
            key,
            value_swapped,
            solved,
            priors,
        ),
    )
    conv_done, conv_part = call(
        conv_kernel,
        "conv",
        [((ROWS, CONV), BF16), ((HALO, CONV), F32)],
        (conv_input, depthwise_taps_weight, conv_gain, conv_shift),
        scratch=[pltpu.VMEM((HALO + ROWS, CONV), F32)],
    )
    for axis, far in (("y", False), ("y", True), ("z", False)):
        other = swapped(pack, axis, 3 if far else 1)
        sent = 1 if axis == "z" else 2
        pack, total, prefix = call(
            functools.partial(pair_kernel, axis, far, sent),
            f"pair_{axis}{3 if far else 1}",
            [((HEAD * sent + HALO // 2, LANES), BF16), state, packed],
            (pack, total, other, prefix),
        )
    other = swapped(pack, "z", 3)
    sends = call(
        last_kernel,
        "last",
        [((SPAN, CONV + LANES), BF16)] * 4,
        (
            other,
            prefix,
            local_read,
            query,
            gate,
            as_row(head_norm_gain),
            conv_done,
            conv_part,
            depthwise_taps_weight,
            conv_gain,
            conv_shift,
        ),
        scratch=[
            pltpu.VMEM((ROWS, CONV + LANES), BF16),
            pltpu.VMEM((2 * HALO, CONV), F32),
        ],
    )
    arrived = [shifted(sends[n], "x", n) for n in (1, 2, 3)]
    (mixed,) = call(
        project_kernel,
        "project",
        [((SPAN, 2048), BF16)],
        (sends[0], *arrived, convolution_output_weight, attention_output_weight),
    )
    return mixed


def solution(mesh):
    split = Mesh(mesh.devices.reshape(4, 4, 2, mesh.shape["tp"]), SP_TP)
    placed = (
        P(SP, None),
        P(),
        P(None, "x"),
        P(None, "x"),
        P(None, "x"),
        P("x"),
        P("x"),
        P(None, "x"),
        P(None, "x"),
        P(None, "x"),
        P(None, "x"),
        P(None, "x"),
        P(None, "x"),
        P("x"),
        P("x"),
        P(SP, "x"),
        P(SP, "x"),
        P("x"),
        P(),
        P(),
    )
    return jax.shard_map(
        local, mesh=split, in_specs=placed, out_specs=P(SP_TP, None), check_vma=False
    )
```

```python
import functools

import jax
import jax.numpy as jnp
from jax import lax
from jax.experimental import pallas as pl
from jax.experimental.pallas import tpu as pltpu
from jax.sharding import Mesh
from jax.sharding import PartitionSpec as P

HEAD = 64
ROWS = 256
LANES = 256
CONV = 128
SPAN = 64
CHUNKS = ROWS // SPAN
HALO = 32
TAPS = 31
PACK = 2 * HEAD + HALO // 2
SP = ("z", "y", "c")
SP_TP = ("z", "y", "c", "x")

NORM_EPS = 1e-06
GROUP_EPS = 1e-05
HEAD_EPS = 0.00064
KEY_EPS = 1e-06
EXP_HALF = 0.6065306597126334

F32 = jnp.float32
BF16 = jnp.bfloat16
NN = (((1,), (0,)), ((), ()))
NT = (((1,), (1,)), ((), ()))
TN = (((0,), (0,)), ((), ()))
VMEM = pl.BlockSpec(memory_space=pltpu.VMEM)
HBM = pl.BlockSpec(memory_space=pltpu.HBM)
ANY = pl.BlockSpec(memory_space=pl.ANY)


def mm(left, right, dims=NN):
    return lax.dot_general(
        left.astype(BF16), right.astype(BF16), dims, preferred_element_type=F32
    )


def halves(value):
    high = value.astype(BF16)
    return high, (value - high.astype(F32)).astype(BF16)


def mm3(left, right, dims=NN):
    left_high, left_low = halves(left)
    right_high, right_low = halves(right)
    return mm(left_high, right_high, dims) + (
        mm(left_high, right_low, dims) + mm(left_low, right_high, dims)
    )


def iota(shape, dim):
    return lax.broadcasted_iota(jnp.int32, shape, dim)


def head_lanes(shape, head):
    return (iota(shape, 1) // HEAD) == head


def block_ones(size):
    shape = (size, size)
    return jnp.where(iota(shape, 0) // HEAD == iota(shape, 1) // HEAD, 1.0, 0.0).astype(BF16)


def group_sum(value, ones):
    high, low = halves(value)
    return mm(high, ones) + mm(low, ones)


def expand(compact):
    shape = (LANES, LANES)
    tall = jnp.concatenate([compact] * (LANES // HEAD), axis=0)
    return jnp.where(iota(shape, 0) // HEAD == iota(shape, 1) // HEAD, tall, 0.0)


def shrink(full):
    parts = [full[HEAD * h : HEAD * (h + 1)] for h in range(LANES // HEAD)]
    return (parts[0] + parts[1]) + (parts[2] + parts[3])


def unit_state():
    shape = (HEAD, LANES)
    eye = jnp.where(iota(shape, 0) == iota(shape, 1) % HEAD, 1.0, 0.0)
    return jnp.concatenate([eye, jnp.zeros(shape, F32)], axis=0)


def follow(earlier, trans, base):
    moved = mm3(earlier, expand(trans))
    return jnp.concatenate([moved[:HEAD], moved[HEAD:] + base], axis=0)


def per_chunk(rows):
    return jnp.concatenate([jnp.broadcast_to(row, (SPAN, LANES)) for row in rows], axis=0)


def swap_pair(value):
    return pltpu.roll(value, HEAD, 1)


def local_kernel(*refs):
    sources = refs[:12]
    pack_out, prior_out, conv_out, normed_out, fall_out, start_out = refs[12:18]
    erase_out, key_out, value_out, solved_out = refs[18:22]
    targets = refs[22:34]
    sems = refs[34]
    copies = [
        pltpu.make_async_copy(source, target, sems.at[n])
        for n, (source, target) in enumerate(zip(sources, targets))
    ]
    for copy in copies:
        copy.start()
    tokens, gain, key_gain, bias, shift, extra = targets[:6]
    copies[0].wait()
    copies[1].wait()
    rows = tokens[...].astype(F32)
    scale = lax.rsqrt(jnp.mean(rows * rows, axis=-1, keepdims=True) + NORM_EPS)
    normed = (rows * scale * gain[...]).astype(BF16)
    normed_out[...] = normed

    def project(n):
        copies[n].wait()
        return rounded_product(normed, targets[n][...])

    square = (ROWS, LANES)
    row_at, lane_at = iota(square, 0), iota(square, 1)
    same_chunk = row_at // SPAN == lane_at // SPAN
    ones = block_ones(LANES)

    key = project(6)
    copies[2].wait()
    key_scaled = key * key_gain[...]
    unit = key_scaled * lax.rsqrt(group_sum(key_scaled * key_scaled, ones) + KEY_EPS)
    erase = unit * jax.nn.sigmoid(project(7))
    decay = project(8)
    for n in (3, 4, 5):
        copies[n].wait()
    logits = decay + bias[...] + shift[...]
    log_decay = extra[...] - EXP_HALF * jax.nn.sigmoid(logits)
    lower = jnp.where(same_chunk & (lane_at <= row_at), 1.0, 0.0).astype(BF16)
    part_high, part_mid = halves(log_decay)
    part_low = (log_decay - part_high.astype(F32) - part_mid.astype(F32)).astype(BF16)
    cumulate = mm(lower, part_high) + (mm(lower, part_mid) + mm(lower, part_low))
    before = cumulate - log_decay
    mids = [cumulate[SPAN * c + 31 : SPAN * c + 32] for c in range(CHUNKS)]
    finals = [cumulate[SPAN * c + 63 : SPAN * c + 64] for c in range(CHUNKS)]
    mid = per_chunk(mids)
    rise = jnp.exp(mid - cumulate)
    fall_out[...] = jnp.exp(cumulate - mid)
    unit_s = unit * jnp.exp(before - mid)
    erase_s = erase * rise
    key_s = key * rise
    starts = [jnp.exp(m) for m in mids]
    for c in range(CHUNKS):
        start_out[c : c + 1] = starts[c]
    to_end = per_chunk([jnp.exp(f - m) for f, m in zip(finals, mids)])
    unit_q = unit_s * per_chunk(starts)
    kept_erase = (erase_s * to_end).astype(BF16)
    kept_key = (key_s * to_end).astype(BF16)
    erase_b = erase_s.astype(BF16)
    key_b = key_s.astype(BF16)
    value = project(9)
    value_b = value.astype(BF16)
    value_swapped = [
        swap_pair(value[:, :128]).astype(BF16),
        swap_pair(value[:, 128:]).astype(BF16),
    ]
    erase_out[...] = erase_b
    key_out[...] = key_b
    value_out[:, :128] = value_swapped[0]
    value_out[:, 128:] = value_swapped[1]

    strict = same_chunk & (lane_at < row_at)
    near = strict & (row_at // 8 == lane_at // 8)
    far = strict & (row_at // 8 != lane_at // 8)
    low_half = iota((ROWS, 128), 1) < HEAD
    solved = []
    for h in range(4):
        pair, own = h // 2, (low_half if h % 2 == 0 else ~low_half)
        span = slice(128 * pair, 128 * pair + 128)
        left = jnp.where(head_lanes(square, h), unit_s, 0.0).astype(BF16)
        erase_mix = mm(left, erase_b, NT)
        key_mix = jnp.where(strict, mm(left, key_b, NT), 0.0)
        d1 = jnp.where(near, erase_mix, 0.0)
        n1 = jnp.where(far, erase_mix, 0.0)
        d2 = mm(d1, d1)
        d4 = mm(d2, d2)
        g = d2 - d1 - mm(d1, d2)
        dinv = g + d4 + mm(g, d4)
        p1 = n1 + mm(dinv, n1)
        p2 = mm(p1, p1)
        p4 = mm(p2, p2)
        key_value = mm(key_mix, value_swapped[pair])
        right = jnp.where(own, unit_q[:, span], key_value)
        y = right + mm(dinv, right)
        y = y + mm(p4, y)
        y = y + mm(p2, y)
        y = mm(p1, y) - y
        solved.append(y)
        solved_out[h] = y.astype(BF16)
    weave = []
    removed = []
    for pair in range(2):
        even, odd = solved[2 * pair], solved[2 * pair + 1]
        weave.append(jnp.where(low_half, even, odd))
        removed.append(swap_pair(jnp.where(low_half, odd, even)))
    weave = jnp.concatenate(weave, axis=1).astype(BF16)
    removed = jnp.concatenate(removed, axis=1).astype(BF16)

    same_head = row_at // HEAD == lane_at // HEAD
    eye = row_at == lane_at
    state = unit_state()
    for c in range(CHUNKS):
        here = slice(SPAN * c, SPAN * c + SPAN)
        prior_out[c] = state
        full = mm(weave[here], kept_erase[here], TN)
        trans = jnp.where(same_head, full, 0.0) + jnp.where(
            eye, jnp.broadcast_to(jnp.exp(finals[c]), square), 0.0
        )
        base = mm(removed[here], kept_erase[here], TN) + mm(value_b[here], kept_key[here], TN)
        base = shrink(jnp.where(same_head, base, 0.0))
        moved = mm3(state, trans)
        state = jnp.concatenate([moved[:HEAD], moved[HEAD:] + base], axis=0)
    pack_out[: 2 * HEAD] = state

    conv_input = rounded(project(10) * jax.nn.sigmoid(project(11)))
    conv_out[...] = conv_input
    pack_out[2 * HEAD :, :128] = conv_input[ROWS - 32 : ROWS - 16]
    pack_out[2 * HEAD :, 128:] = conv_input[ROWS - 16 :]


def rounded(value):
    return value.astype(BF16).astype(F32)


def rounded_product(left, right):
    return rounded(jnp.dot(left, right, preferred_element_type=F32))


def gate_kernel(normed, w_receptance, w_gate, receptance_out, gate_out):
    receptance_out[...] = rounded_product(normed[...], w_receptance[...])
    gate_out[...] = jax.nn.sigmoid(rounded_product(normed[...], w_gate[...]))


def read_kernel(
    receptance,
    fall,
    start,
    erase,
    key,
    value_swapped,
    solved,
    priors,
    local_out,
    query_out,
):
    square = (ROWS, LANES)
    row_at, lane_at = iota(square, 0), iota(square, 1)
    low_half = iota((ROWS, 128), 1) < HEAD
    read_s = receptance[...] * fall[...]
    read_q = read_s * per_chunk([start[c : c + 1] for c in range(CHUNKS)])
    inclusive = (row_at // SPAN == lane_at // SPAN) & (lane_at <= row_at)
    found = []
    for h in range(4):
        pair, own = h // 2, (low_half if h % 2 == 0 else ~low_half)
        span = slice(128 * pair, 128 * pair + 128)
        left = jnp.where(head_lanes(square, h), read_s, 0.0).astype(BF16)
        read_erase = jnp.where(inclusive, mm(left, erase[...], NT), 0.0)
        read_key = jnp.where(inclusive, mm(left, key[...], NT), 0.0)
        mine = jnp.where(own, 0.0, value_swapped[:, span].astype(F32))
        found.append(mm(read_erase, solved[h]) + mm(read_key, mine))
    query, local = [], []
    for pair in range(2):
        even, odd = found[2 * pair], found[2 * pair + 1]
        query.append(jnp.where(low_half, even, odd))
        local.append(swap_pair(jnp.where(low_half, odd, even)))
    query = jnp.concatenate(query, axis=1) + read_q
    local = jnp.concatenate(local, axis=1)
    for c in range(CHUNKS):
        here = slice(SPAN * c, SPAN * c + SPAN)
        if c == 0:
            local_out[here] = local[here]
            query_out[here] = query[here].astype(BF16)
        else:
            prior = priors[c]
            local_out[here] = local[here] + mm(query[here], expand(prior[HEAD:]), NT)
            query_out[here] = mm(query[here], expand(prior[:HEAD]), NT).astype(BF16)


def conv_kernel(conv_in, taps, gain, shift, done_out, part_out, padded):
    padded[:HALO] = jnp.zeros((HALO, CONV), F32)
    padded[HALO:] = conv_in[...]
    total = jnp.zeros((ROWS, CONV), F32)
    for j in range(TAPS):
        total = total + taps[j : j + 1] * padded[2 + j : 2 + j + ROWS]
    part_out[...] = total[:HALO]
    done_out[...] = finish_conv(total, gain[...], shift[...])


def finish_conv(total, gain, shift):
    ones = block_ones(CONV)
    centred = total - group_sum(total, ones) * (1.0 / HEAD)
    spread = group_sum(centred * centred, ones) * (1.0 / HEAD)
    scaled = centred * lax.rsqrt(spread + GROUP_EPS) * gain + shift
    return (scaled * jax.nn.sigmoid(scaled)).astype(BF16)


def joined(lower, upper):
    return follow(lower[: 2 * HEAD], upper[:HEAD], upper[HEAD : 2 * HEAD])


def core_kernel(mine, other, pack_out, prefix_out, total_out):
    first = lax.axis_index("c") == 0
    early = jnp.where(first, mine[...], other[...])
    late = jnp.where(first, other[...], mine[...])
    total = joined(early, late)
    total_out[...] = total
    pack_out[: 2 * HEAD] = total.astype(BF16)
    pack_out[2 * HEAD :] = late[2 * HEAD :].astype(BF16)
    prefix_out[: 2 * HEAD] = jnp.where(first, unit_state(), early[: 2 * HEAD])
    prefix_out[2 * HEAD :] = jnp.where(first, 0.0, early[2 * HEAD :])


def pair_kernel(axis, far, sent, mine, total, other, prefix, _, pack_out, prefix_out, *total_out):
    at = lax.axis_index(axis)
    upper = (at >= 2) if far else (lax.rem(at, 2) == 1)
    got = other[...].astype(F32)
    states = got[: 2 * HEAD]
    early = jnp.where(upper, states, total[...])
    late = jnp.where(upper, total[...], states)
    result = joined(early, late)
    for out in total_out:
        out[...] = result
    pack_out[: HEAD * sent] = result[HEAD * (2 - sent) :].astype(BF16)
    tail = other if far else mine
    pack_out[HEAD * sent :] = tail[2 * HEAD :]
    behind = joined(states, prefix[...])
    prefix_out[: 2 * HEAD] = jnp.where(upper, behind, prefix[: 2 * HEAD])
    takes = (at == 2) if far else upper
    takes = takes & (lax.axis_index("c") == 0)
    if axis == "z":
        takes = takes & (lax.axis_index("y") == 0)
    prefix_out[2 * HEAD :] = jnp.where(takes, got[2 * HEAD :], prefix[2 * HEAD :])


def last_kernel(
    other,
    prefix,
    local,
    query,
    gate,
    head_gain,
    conv_done,
    conv_part,
    taps,
    conv_gain,
    conv_shift,
    out_0,
    out_1,
    out_2,
    out_3,
    ready,
    padded,
):
    z, y, c, x = (lax.axis_index(name) for name in SP_TP)
    got = other[...].astype(F32)
    entering = jnp.where(z >= 2, got[:HEAD], 0.0)
    state = mm3(entering, expand(prefix[:HEAD])) + prefix[HEAD : 2 * HEAD]
    readout = local[...] + mm(query[...], expand(state), NT)
    ones = block_ones(LANES)
    centred = readout - group_sum(readout, ones) * (1.0 / HEAD)
    spread = group_sum(centred * centred, ones) * (1.0 / HEAD)
    mixed = centred * lax.rsqrt(spread + HEAD_EPS) * head_gain[...] * gate[...]
    ready[:, CONV:] = mixed.astype(BF16)
    ready[:, :CONV] = conv_done[...]

    takes = (z == 2) & (y == 0) & (c == 0)
    side = jnp.where(takes, got[HEAD:], prefix[2 * HEAD :])
    padded[:16] = side[:, :128]
    padded[16:32] = side[:, 128:]
    padded[32:] = jnp.zeros((HALO, CONV), F32)
    total = conv_part[...]
    for j in range(TAPS):
        total = total + taps[j : j + 1] * padded[2 + j : 2 + j + HALO]
    ready[:HALO, :CONV] = finish_conv(total, conv_gain[...], conv_shift[...])
    for n, out in enumerate((out_0, out_1, out_2, out_3)):
        to = lax.rem(x + n, 4)
        out[...] = ready[pl.ds(pl.multiple_of(to * SPAN, SPAN), SPAN)]


def project_kernel(own, from_1, from_2, from_3, conv_w, mix_w, out, conv_rows, mix_rows):
    x = lax.axis_index("x")
    for n, ref in enumerate((own, from_1, from_2, from_3)):
        of = lax.rem(x - n + 4, 4)
        conv_rows[:, pl.ds(pl.multiple_of(of * CONV, CONV), CONV)] = ref[:, :CONV]
        mix_rows[:, pl.ds(pl.multiple_of(of * LANES, LANES), LANES)] = ref[:, CONV:]
    total = jnp.dot(conv_rows[...], conv_w[...], preferred_element_type=F32)
    total = total + jnp.dot(mix_rows[...], mix_w[...], preferred_element_type=F32)
    out[...] = total.astype(BF16)


def shifted(value, axis, steps):
    count = lax.axis_size(axis)
    return lax.ppermute(value, axis, [(s, (s + steps) % count) for s in range(count)])


def swapped(value, axis, bits):
    count = lax.axis_size(axis)
    return lax.ppermute(value, axis, [(s, s ^ bits) for s in range(count)])


def params():
    return pltpu.CompilerParams(vmem_limit_bytes=40 * 1024 * 1024)


def call(kernel, name, outs, arguments, specs=None, scratch=(), pinned=False):
    if pinned:
        arguments = [pltpu.with_memory_space_constraint(a, pltpu.HBM) for a in arguments]
    return pl.pallas_call(
        kernel,
        name=name,
        out_shape=[jax.ShapeDtypeStruct(*o) for o in outs],
        in_specs=specs or [VMEM] * len(arguments),
        out_specs=[VMEM] * len(outs),
        scratch_shapes=list(scratch),
        compiler_params=params(),
    )(*arguments)


def local(
    tokens,
    input_norm_gain,
    convolution_value_weight,
    convolution_gate_weight,
    depthwise_taps_weight,
    convolution_group_gain,
    convolution_group_shift,
    receptance_weight,
    key_weight,
    value_weight,
    decay_weight,
    correction_rate_weight,
    output_gate_weight,
    key_prenorm_gain,
    decay_offset_bias,
    position_decay_shift,
    extra_log_decay,
    head_norm_gain,
    convolution_output_weight,
    attention_output_weight,
):
    def as_row(value):
        return value.reshape(1, value.shape[0])

    conv_gain, conv_shift = as_row(convolution_group_gain), as_row(convolution_group_shift)
    wide = pltpu.VMEM((2048, LANES), BF16)
    thin = pltpu.VMEM((2048, CONV), BF16)
    row = pltpu.VMEM((1, LANES), F32)
    square = ((ROWS, LANES), F32)
    square_b = ((ROWS, LANES), BF16)
    state = ((2 * HEAD, LANES), F32)
    packed = ((PACK, LANES), F32)
    packed_b = ((PACK, LANES), BF16)
    pack, priors, conv_input, normed, fall, start, erase, key, value_swapped, solved = call(
        local_kernel,
        "local",
        [
            packed,
            ((CHUNKS, 2 * HEAD, LANES), F32),
            ((ROWS, CONV), F32),
            ((ROWS, 2048), BF16),
            square,
            ((8, LANES), F32),
            square_b,
            square_b,
            square_b,
            ((4, ROWS, CONV), BF16),
        ],
        (
            tokens,
            as_row(input_norm_gain),
            as_row(key_prenorm_gain),
            as_row(decay_offset_bias),
            position_decay_shift,
            extra_log_decay,
            key_weight,
            correction_rate_weight,
            decay_weight,
            value_weight,
            convolution_value_weight,
            convolution_gate_weight,
        ),
        specs=[HBM] * 12,
        pinned=True,
        scratch=[pltpu.VMEM((ROWS, 2048), BF16), pltpu.VMEM((1, 2048), F32), row, row]
        + [pltpu.VMEM((ROWS, LANES), F32)] * 2
        + [wide] * 4
        + [thin] * 2
        + [pltpu.SemaphoreType.DMA((12,))],
    )
    other = swapped(pack, "c", 1)
    pack, prefix, *total = call(core_kernel, "core", [packed_b, packed, state], (pack, other))
    receptance, gate = call(
        gate_kernel,
        "gate",
        [square, square],
        (normed, receptance_weight, output_gate_weight),
    )
    local_read, query = call(
        read_kernel,
        "read",
        [square, square_b],
        (receptance, fall, start, erase, key, value_swapped, solved, priors),
    )
    conv_done, conv_part = call(
        conv_kernel,
        "conv",
        [((ROWS, CONV), BF16), ((HALO, CONV), F32)],
        (conv_input, depthwise_taps_weight, conv_gain, conv_shift),
        scratch=[pltpu.VMEM((HALO + ROWS, CONV), F32)],
    )
    beside = (conv_done, receptance, local_read)
    for (axis, far), side in zip((("y", False), ("y", True), ("z", False)), beside):
        other = swapped(pack, axis, 3 if far else 1)
        sent = 1 if axis == "z" else 2
        pack, prefix, *total = call(
            functools.partial(pair_kernel, axis, far, sent),
            f"pair_{axis}{3 if far else 1}",
            [((HEAD * sent + HALO // 2, LANES), BF16), packed] + [state] * (sent - 1),
            (pack, total[0], other, prefix, side),
            specs=[VMEM] * 4 + [ANY],
        )
    other = swapped(pack, "z", 3)
    sends = call(
        last_kernel,
        "last",
        [((SPAN, CONV + LANES), BF16)] * 4,
        (
            other,
            prefix,
            local_read,
            query,
            gate,
            as_row(head_norm_gain),
            conv_done,
            conv_part,
            depthwise_taps_weight,
            conv_gain,
            conv_shift,
        ),
        scratch=[
            pltpu.VMEM((ROWS, CONV + LANES), BF16),
            pltpu.VMEM((2 * HALO, CONV), F32),
        ],
    )
    arrived = [shifted(sends[n], "x", n) for n in (1, 2, 3)]
    (mixed,) = call(
        project_kernel,
        "project",
        [((SPAN, 2048), BF16)],
        (sends[0], *arrived, convolution_output_weight, attention_output_weight),
        scratch=[pltpu.VMEM((SPAN, 512), BF16), pltpu.VMEM((SPAN, 1024), BF16)],
    )
    return mixed


def solution(mesh):
    split = Mesh(mesh.devices.reshape(4, 4, 2, mesh.shape["tp"]), SP_TP)
    placed = (
        P(SP, None),
        P(),
        P(None, "x"),
        P(None, "x"),
        P(None, "x"),
        P("x"),
        P("x"),
        P(None, "x"),
        P(None, "x"),
        P(None, "x"),
        P(None, "x"),
        P(None, "x"),
        P(None, "x"),
        P("x"),
        P("x"),
        P(SP, "x"),
        P(SP, "x"),
        P("x"),
        P(),
        P(),
    )
    return jax.shard_map(
        local, mesh=split, in_specs=placed, out_specs=P(SP_TP, None), check_vma=False
    )
```

```python
import functools

import jax
import jax.numpy as jnp
from jax import lax
from jax.experimental import pallas as pl
from jax.experimental.pallas import tpu as pltpu
from jax.sharding import Mesh
from jax.sharding import PartitionSpec as P

HEAD = 64
ROWS = 256
LANES = 256
CONV = 128
SPAN = 64
CHUNKS = ROWS // SPAN
HALO = 32
TAPS = 31
PACK = 2 * HEAD + HALO // 2
SP = ("z", "y", "c")
SP_TP = ("z", "y", "c", "x")

NORM_EPS = 1e-06
GROUP_EPS = 1e-05
HEAD_EPS = 0.00064
KEY_EPS = 1e-06
EXP_HALF = 0.6065306597126334

F32 = jnp.float32
BF16 = jnp.bfloat16
NN = (((1,), (0,)), ((), ()))
NT = (((1,), (1,)), ((), ()))
TN = (((0,), (0,)), ((), ()))
VMEM = pl.BlockSpec(memory_space=pltpu.VMEM)
HBM = pl.BlockSpec(memory_space=pltpu.HBM)
ANY = pl.BlockSpec(memory_space=pl.ANY)


def mm(left, right, dims=NN):
    return lax.dot_general(
        left.astype(BF16), right.astype(BF16), dims, preferred_element_type=F32
    )


def halves(value):
    high = value.astype(BF16)
    return high, (value - high.astype(F32)).astype(BF16)


def mm3(left, right, dims=NN):
    left_high, left_low = halves(left)
    right_high, right_low = halves(right)
    return mm(left_high, right_high, dims) + (
        mm(left_high, right_low, dims) + mm(left_low, right_high, dims)
    )


def iota(shape, dim):
    return lax.broadcasted_iota(jnp.int32, shape, dim)


def head_lanes(shape, head):
    return (iota(shape, 1) // HEAD) == head


def block_ones(size):
    shape = (size, size)
    return jnp.where(iota(shape, 0) // HEAD == iota(shape, 1) // HEAD, 1.0, 0.0).astype(BF16)


def group_sum(value, ones):
    high, low = halves(value)
    return mm(high, ones) + mm(low, ones)


def expand(compact):
    shape = (LANES, LANES)
    tall = jnp.concatenate([compact] * (LANES // HEAD), axis=0)
    return jnp.where(iota(shape, 0) // HEAD == iota(shape, 1) // HEAD, tall, 0.0)


def shrink(full):
    parts = [full[HEAD * h : HEAD * (h + 1)] for h in range(LANES // HEAD)]
    return (parts[0] + parts[1]) + (parts[2] + parts[3])


def unit_state():
    shape = (HEAD, LANES)
    eye = jnp.where(iota(shape, 0) == iota(shape, 1) % HEAD, 1.0, 0.0)
    return jnp.concatenate([eye, jnp.zeros(shape, F32)], axis=0)


def follow(earlier, trans, base):
    moved = mm3(earlier, expand(trans))
    return jnp.concatenate([moved[:HEAD], moved[HEAD:] + base], axis=0)


def per_chunk(rows):
    return jnp.concatenate([jnp.broadcast_to(row, (SPAN, LANES)) for row in rows], axis=0)


def swap_pair(value):
    return pltpu.roll(value, HEAD, 1)


def local_kernel(*refs):
    sources = refs[:14]
    pack_out, prior_out, conv_out, normed, fall_out, start_out = refs[14:20]
    erase_out, key_out, value_out, weave_out, removed_out = refs[20:25]
    late_weights = refs[25:27]
    tokens, gain, key_gain, bias, shift, extra = refs[27:33]
    weights = refs[33:37]
    conv_weights = refs[37]
    sems = refs[38]
    targets = (
        tokens,
        gain,
        key_gain,
        bias,
        shift,
        extra,
        *weights,
        conv_weights.at[:, :CONV],
        conv_weights.at[:, CONV:],
        *late_weights,
    )
    copies = [
        pltpu.make_async_copy(source, target, sems.at[n])
        for n, (source, target) in enumerate(zip(sources, targets))
    ]
    for n in (0, 1, 6, 2, 7, 8, 3, 4, 5, 9, 10, 11, 12, 13):
        copies[n].start()
    copies[0].wait()
    copies[1].wait()
    for n in range(ROWS // 16):
        here = slice(16 * n, 16 * n + 16)
        rows = tokens[here].astype(F32)
        scale = lax.rsqrt(jnp.mean(rows * rows, axis=-1, keepdims=True) + NORM_EPS)
        normed[here] = (rows * scale * gain[...]).astype(BF16)

    def project(n):
        copies[n].wait()
        return rounded_product(normed[...], targets[n][...])

    square = (ROWS, LANES)
    row_at, lane_at = iota(square, 0), iota(square, 1)
    ones = block_ones(LANES)

    key = project(6)
    copies[2].wait()
    key_scaled = key * key_gain[...]
    unit = key_scaled * lax.rsqrt(group_sum(key_scaled * key_scaled, ones) + KEY_EPS)
    erase = unit * jax.nn.sigmoid(project(7))
    decay = project(8)
    for n in (3, 4, 5):
        copies[n].wait()
    logits = decay + bias[...] + shift[...]
    log_decay = extra[...] - EXP_HALF * jax.nn.sigmoid(logits)
    small = (SPAN, SPAN)
    lower = jnp.where(iota(small, 1) <= iota(small, 0), 1.0, 0.0).astype(BF16)
    part_high, part_mid = halves(log_decay)
    part_low = (log_decay - part_high.astype(F32) - part_mid.astype(F32)).astype(BF16)
    chunks = [slice(SPAN * c, SPAN * c + SPAN) for c in range(CHUNKS)]
    cumulate = jnp.concatenate(
        [
            mm(lower, part_high[at]) + (mm(lower, part_mid[at]) + mm(lower, part_low[at]))
            for at in chunks
        ],
        axis=0,
    )
    before = cumulate - log_decay
    mids = [cumulate[SPAN * c + 31 : SPAN * c + 32] for c in range(CHUNKS)]
    finals = [cumulate[SPAN * c + 63 : SPAN * c + 64] for c in range(CHUNKS)]
    mid = per_chunk(mids)
    rise = jnp.exp(mid - cumulate)
    fall_out[...] = jnp.exp(cumulate - mid)
    unit_s = unit * jnp.exp(before - mid)
    erase_s = erase * rise
    key_s = key * rise
    starts = [jnp.exp(m) for m in mids]
    for c in range(CHUNKS):
        start_out[c : c + 1] = starts[c]
    to_end = per_chunk([jnp.exp(f - m) for f, m in zip(finals, mids)])
    unit_q = unit_s * per_chunk(starts)
    kept_erase = (erase_s * to_end).astype(BF16)
    kept_key = (key_s * to_end).astype(BF16)
    erase_b = erase_s.astype(BF16)
    key_b = key_s.astype(BF16)
    unit_b = unit_s.astype(BF16)
    value_b = project(9).astype(BF16)
    erase_out[...] = erase_b
    key_out[...] = key_b
    value_out[...] = value_b

    copies[10].wait()
    copies[11].wait()
    both = rounded_product(normed[...], conv_weights[...])
    conv_input = rounded(both[:, :CONV] * jax.nn.sigmoid(both[:, CONV:]))
    conv_out[...] = conv_input
    pack_out[2 * HEAD :, :128] = conv_input[ROWS - 32 : ROWS - 16]
    pack_out[2 * HEAD :, 128:] = conv_input[ROWS - 16 :]

    flat = (SPAN, LANES)
    row_in, lane_in = iota(flat, 0), iota(flat, 1) % HEAD
    strict = lane_in < row_in
    near = strict & (row_in // 8 == lane_in // 8)
    far = strict & (row_in // 8 != lane_in // 8)

    def spread(value):
        return jnp.concatenate([value.astype(BF16)] * 4, axis=0) * ones

    def times(left, right):
        return [mm(x, spread(y)) for x, y in zip(left, right)]

    def add(*terms):
        return [functools.reduce(lambda p, q: p + q, group) for group in zip(*terms)]

    erase_mix = [mm(unit_b[at], spread(erase_b[at]), NT) for at in chunks]
    key_mix = [
        jnp.where(strict, mm(unit_b[at], spread(key_b[at]), NT), 0.0) for at in chunks
    ]
    d1 = [jnp.where(near, a, 0.0) for a in erase_mix]
    n1 = [jnp.where(far, a, 0.0) for a in erase_mix]
    d2 = times(d1, d1)
    key_value = times(key_mix, [value_b[at] for at in chunks])
    stacked = times([jnp.concatenate([p, q], axis=0) for p, q in zip(d1, d2)], d2)
    d4 = [m[SPAN:] for m in stacked]
    g = [q - p - m[:SPAN] for p, q, m in zip(d1, d2, stacked)]
    dinv = add(g, d4, times(g, d4))
    p1 = add(n1, times(dinv, n1))
    p2 = times(p1, p1)
    m1 = [d - p - r for d, p, r in zip(dinv, p1, times(p1, dinv))]
    p4 = times(p2, p2)
    m2 = add(m1, p2, times(p2, m1))
    m3 = add(m2, p4, times(p4, m2))
    start_unit = [unit_q[at] for at in chunks]
    weave = [-x for x in add(start_unit, times(m3, start_unit))]
    removed = [-x for x in add(key_value, times(m3, key_value))]
    weave = [x.astype(BF16) for x in weave]
    removed = [x.astype(BF16) for x in removed]

    same_head = row_at // HEAD == lane_at // HEAD
    eye = row_at == lane_at
    state = unit_state()
    for c, at in enumerate(chunks):
        weave_out[at] = weave[c]
        removed_out[at] = removed[c]
        prior_out[c] = state
        trans = jnp.where(same_head, mm(weave[c], kept_erase[at], TN), 0.0) + jnp.where(
            eye, jnp.broadcast_to(jnp.exp(finals[c]), square), 0.0
        )
        base = mm(
            jnp.concatenate([removed[c], value_b[at]], axis=0),
            jnp.concatenate([kept_erase[at], kept_key[at]], axis=0),
            TN,
        )
        base = shrink(jnp.where(same_head, base, 0.0))
        if c == 0:
            state = jnp.concatenate([shrink(trans), base], axis=0)
        else:
            moved = mm3(state, trans)
            state = jnp.concatenate([moved[:HEAD], moved[HEAD:] + base], axis=0)
    pack_out[: 2 * HEAD] = state
    copies[12].wait()
    copies[13].wait()


def rounded(value):
    return value.astype(BF16).astype(F32)


def rounded_product(left, right):
    return rounded(jnp.dot(left, right, preferred_element_type=F32))


def gate_kernel(normed, w_receptance, w_gate, receptance_out, gate_out):
    receptance_out[...] = rounded_product(normed[...], w_receptance[...])
    gate_out[...] = jax.nn.sigmoid(rounded_product(normed[...], w_gate[...]))


def read_kernel(
    receptance,
    fall,
    start,
    erase,
    key,
    value,
    weave,
    removed,
    priors,
    local_out,
    query_out,
):
    ones = block_ones(LANES)
    flat = (SPAN, LANES)
    inclusive = iota(flat, 1) % HEAD <= iota(flat, 0)

    def spread(part):
        return jnp.concatenate([part.astype(BF16)] * 4, axis=0) * ones

    for c in range(CHUNKS):
        here = slice(SPAN * c, SPAN * c + SPAN)
        read_s = receptance[here] * fall[here]
        read_b = read_s.astype(BF16)
        read_erase = jnp.where(inclusive, mm(read_b, spread(erase[here]), NT), 0.0)
        read_key = jnp.where(inclusive, mm(read_b, spread(key[here]), NT), 0.0)
        query = read_s * start[c : c + 1] + mm(read_erase, spread(weave[here]))
        local = mm(read_erase, spread(removed[here])) + mm(read_key, spread(value[here]))
        if c:
            prior = priors[c]
            local = local + mm(query, spread(prior[HEAD:]), NT)
            query = mm(query, spread(prior[:HEAD]), NT)
        local_out[here] = local
        query_out[here] = query.astype(BF16)


def conv_kernel(conv_in, taps, gain, shift, done_out, part_out, padded):
    padded[:HALO] = jnp.zeros((HALO, CONV), F32)
    padded[HALO:] = conv_in[...]
    total = jnp.zeros((ROWS, CONV), F32)
    for j in range(TAPS):
        total = total + taps[j : j + 1] * padded[2 + j : 2 + j + ROWS]
    part_out[...] = total[:HALO]
    done_out[...] = finish_conv(total, gain[...], shift[...])


def finish_conv(total, gain, shift):
    ones = block_ones(CONV)
    centred = total - group_sum(total, ones) * (1.0 / HEAD)
    spread = group_sum(centred * centred, ones) * (1.0 / HEAD)
    scaled = centred * lax.rsqrt(spread + GROUP_EPS) * gain + shift
    return (scaled * jax.nn.sigmoid(scaled)).astype(BF16)


def joined(lower, upper):
    return follow(lower[: 2 * HEAD], upper[:HEAD], upper[HEAD : 2 * HEAD])


def core_kernel(mine, other, pack_out, prefix_out, total_out):
    first = lax.axis_index("c") == 0
    early = jnp.where(first, mine[...], other[...])
    late = jnp.where(first, other[...], mine[...])
    total = joined(early, late)
    total_out[...] = total
    pack_out[: 2 * HEAD] = total.astype(BF16)
    pack_out[2 * HEAD :] = late[2 * HEAD :].astype(BF16)
    prefix_out[: 2 * HEAD] = jnp.where(first, unit_state(), early[: 2 * HEAD])
    prefix_out[2 * HEAD :] = jnp.where(first, 0.0, early[2 * HEAD :])


def pair_kernel(axis, far, sent, mine, total, other, prefix, _, pack_out, prefix_out, *total_out):
    at = lax.axis_index(axis)
    upper = (at >= 2) if far else (lax.rem(at, 2) == 1)
    got = other[...].astype(F32)
    states = got[: 2 * HEAD]
    early = jnp.where(upper, states, total[...])
    late = jnp.where(upper, total[...], states)
    result = joined(early, late)
    for out in total_out:
        out[...] = result
    pack_out[: HEAD * sent] = result[HEAD * (2 - sent) :].astype(BF16)
    tail = other if far else mine
    pack_out[HEAD * sent :] = tail[2 * HEAD :]
    behind = joined(states, prefix[...])
    prefix_out[: 2 * HEAD] = jnp.where(upper, behind, prefix[: 2 * HEAD])
    takes = (at == 2) if far else upper
    takes = takes & (lax.axis_index("c") == 0)
    if axis == "z":
        takes = takes & (lax.axis_index("y") == 0)
    prefix_out[2 * HEAD :] = jnp.where(takes, got[2 * HEAD :], prefix[2 * HEAD :])


def last_kernel(
    other,
    prefix,
    local,
    query,
    gate,
    head_gain,
    conv_done,
    conv_part,
    taps,
    conv_gain,
    conv_shift,
    out_0,
    out_1,
    out_2,
    out_3,
    ready,
    padded,
):
    z, y, c, x = (lax.axis_index(name) for name in SP_TP)
    got = other[...].astype(F32)
    entering = jnp.where(z >= 2, got[:HEAD], 0.0)
    state = mm3(entering, expand(prefix[:HEAD])) + prefix[HEAD : 2 * HEAD]
    readout = local[...] + mm(query[...], expand(state), NT)
    ones = block_ones(LANES)
    centred = readout - group_sum(readout, ones) * (1.0 / HEAD)
    spread = group_sum(centred * centred, ones) * (1.0 / HEAD)
    mixed = centred * lax.rsqrt(spread + HEAD_EPS) * head_gain[...] * gate[...]
    ready[:, CONV:] = mixed.astype(BF16)
    ready[:, :CONV] = conv_done[...]

    takes = (z == 2) & (y == 0) & (c == 0)
    side = jnp.where(takes, got[HEAD:], prefix[2 * HEAD :])
    padded[:16] = side[:, :128]
    padded[16:32] = side[:, 128:]
    padded[32:] = jnp.zeros((HALO, CONV), F32)
    total = conv_part[...]
    for j in range(TAPS):
        total = total + taps[j : j + 1] * padded[2 + j : 2 + j + HALO]
    ready[:HALO, :CONV] = finish_conv(total, conv_gain[...], conv_shift[...])
    for n, out in enumerate((out_0, out_1, out_2, out_3)):
        to = lax.rem(x + n, 4)
        out[...] = ready[pl.ds(pl.multiple_of(to * SPAN, SPAN), SPAN)]


def project_kernel(own, from_1, from_2, from_3, conv_w, mix_w, out, conv_rows, mix_rows):
    x = lax.axis_index("x")
    for n, ref in enumerate((own, from_1, from_2, from_3)):
        of = lax.rem(x - n + 4, 4)
        conv_rows[:, pl.ds(pl.multiple_of(of * CONV, CONV), CONV)] = ref[:, :CONV]
        mix_rows[:, pl.ds(pl.multiple_of(of * LANES, LANES), LANES)] = ref[:, CONV:]
    total = jnp.dot(conv_rows[...], conv_w[...], preferred_element_type=F32)
    total = total + jnp.dot(mix_rows[...], mix_w[...], preferred_element_type=F32)
    out[...] = total.astype(BF16)


def shifted(value, axis, steps):
    count = lax.axis_size(axis)
    return lax.ppermute(value, axis, [(s, (s + steps) % count) for s in range(count)])


def swapped(value, axis, bits):
    count = lax.axis_size(axis)
    return lax.ppermute(value, axis, [(s, s ^ bits) for s in range(count)])


def params():
    return pltpu.CompilerParams(vmem_limit_bytes=40 * 1024 * 1024)


def call(kernel, name, outs, arguments, specs=None, scratch=(), pinned=False):
    if pinned:
        arguments = [pltpu.with_memory_space_constraint(a, pltpu.HBM) for a in arguments]
    return pl.pallas_call(
        kernel,
        name=name,
        out_shape=[jax.ShapeDtypeStruct(*o) for o in outs],
        in_specs=specs or [VMEM] * len(arguments),
        out_specs=[VMEM] * len(outs),
        scratch_shapes=list(scratch),
        compiler_params=params(),
    )(*arguments)


def local(
    tokens,
    input_norm_gain,
    convolution_value_weight,
    convolution_gate_weight,
    depthwise_taps_weight,
    convolution_group_gain,
    convolution_group_shift,
    receptance_weight,
    key_weight,
    value_weight,
    decay_weight,
    correction_rate_weight,
    output_gate_weight,
    key_prenorm_gain,
    decay_offset_bias,
    position_decay_shift,
    extra_log_decay,
    head_norm_gain,
    convolution_output_weight,
    attention_output_weight,
):
    def as_row(value):
        return value.reshape(1, value.shape[0])

    conv_gain, conv_shift = as_row(convolution_group_gain), as_row(convolution_group_shift)
    wide = pltpu.VMEM((2048, LANES), BF16)
    row = pltpu.VMEM((1, LANES), F32)
    square = ((ROWS, LANES), F32)
    square_b = ((ROWS, LANES), BF16)
    state = ((2 * HEAD, LANES), F32)
    packed = ((PACK, LANES), F32)
    packed_b = ((PACK, LANES), BF16)
    (
        pack,
        priors,
        conv_input,
        normed,
        fall,
        start,
        erase,
        key,
        value,
        weave,
        removed,
        w_receptance,
        w_gate,
    ) = call(
        local_kernel,
        "local",
        [
            packed,
            ((CHUNKS, 2 * HEAD, LANES), F32),
            ((ROWS, CONV), F32),
            ((ROWS, 2048), BF16),
            square,
            ((8, LANES), F32),
        ]
        + [square_b] * 5
        + [((2048, LANES), BF16)] * 2,
        (
            tokens,
            as_row(input_norm_gain),
            as_row(key_prenorm_gain),
            as_row(decay_offset_bias),
            position_decay_shift,
            extra_log_decay,
            key_weight,
            correction_rate_weight,
            decay_weight,
            value_weight,
            convolution_value_weight,
            convolution_gate_weight,
            receptance_weight,
            output_gate_weight,
        ),
        specs=[HBM] * 14,
        pinned=True,
        scratch=[pltpu.VMEM((ROWS, 2048), BF16), pltpu.VMEM((1, 2048), F32), row, row]
        + [pltpu.VMEM((ROWS, LANES), F32)] * 2
        + [wide] * 5
        + [pltpu.SemaphoreType.DMA((14,))],
    )
    other = swapped(pack, "c", 1)
    pack, prefix, *total = call(core_kernel, "core", [packed_b, packed, state], (pack, other))
    receptance, gate = call(
        gate_kernel,
        "gate",
        [square, square],
        (normed, w_receptance, w_gate),
    )
    local_read, query = call(
        read_kernel,
        "read",
        [square, square_b],
        (receptance, fall, start, erase, key, value, weave, removed, priors),
    )
    conv_done, conv_part = call(
        conv_kernel,
        "conv",
        [((ROWS, CONV), BF16), ((HALO, CONV), F32)],
        (conv_input, depthwise_taps_weight, conv_gain, conv_shift),
        scratch=[pltpu.VMEM((HALO + ROWS, CONV), F32)],
    )
    beside = (conv_done, receptance, local_read)
    for (axis, far), side in zip((("y", False), ("y", True), ("z", False)), beside):
        other = swapped(pack, axis, 3 if far else 1)
        sent = 1 if axis == "z" else 2
        pack, prefix, *total = call(
            functools.partial(pair_kernel, axis, far, sent),
            f"pair_{axis}{3 if far else 1}",
            [((HEAD * sent + HALO // 2, LANES), BF16), packed] + [state] * (sent - 1),
            (pack, total[0], other, prefix, side),
            specs=[VMEM] * 4 + [ANY],
        )
    other = swapped(pack, "z", 3)
    sends = call(
        last_kernel,
        "last",
        [((SPAN, CONV + LANES), BF16)] * 4,
        (
            other,
            prefix,
            local_read,
            query,
            gate,
            as_row(head_norm_gain),
            conv_done,
            conv_part,
            depthwise_taps_weight,
            conv_gain,
            conv_shift,
        ),
        scratch=[
            pltpu.VMEM((ROWS, CONV + LANES), BF16),
            pltpu.VMEM((2 * HALO, CONV), F32),
        ],
    )
    arrived = [shifted(sends[n], "x", n) for n in (1, 2, 3)]
    (mixed,) = call(
        project_kernel,
        "project",
        [((SPAN, 2048), BF16)],
        (sends[0], *arrived, convolution_output_weight, attention_output_weight),
        scratch=[pltpu.VMEM((SPAN, 512), BF16), pltpu.VMEM((SPAN, 1024), BF16)],
    )
    return mixed


def solution(mesh):
    split = Mesh(mesh.devices.reshape(4, 4, 2, mesh.shape["tp"]), SP_TP)
    placed = (
        P(SP, None),
        P(),
        P(None, "x"),
        P(None, "x"),
        P(None, "x"),
        P("x"),
        P("x"),
        P(None, "x"),
        P(None, "x"),
        P(None, "x"),
        P(None, "x"),
        P(None, "x"),
        P(None, "x"),
        P("x"),
        P("x"),
        P(SP, "x"),
        P(SP, "x"),
        P("x"),
        P(),
        P(),
    )
    return jax.shard_map(
        local, mesh=split, in_specs=placed, out_specs=P(SP_TP, None), check_vma=False
    )
```

```python
import functools

import jax
import jax.numpy as jnp
from jax import lax
from jax.experimental import pallas as pl
from jax.experimental.pallas import tpu as pltpu
from jax.sharding import Mesh
from jax.sharding import PartitionSpec as P

HEAD = 64
ROWS = 256
LANES = 256
CONV = 128
SPAN = 64
CHUNKS = ROWS // SPAN
HALO = 32
TAPS = 31
PACK = 2 * HEAD + HALO // 2
SP = ("z", "y", "c")
SP_TP = ("z", "y", "c", "x")

NORM_EPS = 1e-06
GROUP_EPS = 1e-05
HEAD_EPS = 0.00064
KEY_EPS = 1e-06
EXP_HALF = 0.6065306597126334

F32 = jnp.float32
BF16 = jnp.bfloat16
NN = (((1,), (0,)), ((), ()))
NT = (((1,), (1,)), ((), ()))
TN = (((0,), (0,)), ((), ()))
VMEM = pl.BlockSpec(memory_space=pltpu.VMEM)
HBM = pl.BlockSpec(memory_space=pltpu.HBM)
ANY = pl.BlockSpec(memory_space=pl.ANY)


def mm(left, right, dims=NN):
    return lax.dot_general(
        left.astype(BF16), right.astype(BF16), dims, preferred_element_type=F32
    )


def halves(value):
    high = value.astype(BF16)
    return high, (value - high.astype(F32)).astype(BF16)


def mm3(left, right, dims=NN):
    left_high, left_low = halves(left)
    right_high, right_low = halves(right)
    return mm(left_high, right_high, dims) + (
        mm(left_high, right_low, dims) + mm(left_low, right_high, dims)
    )


def iota(shape, dim):
    return lax.broadcasted_iota(jnp.int32, shape, dim)


def head_lanes(shape, head):
    return (iota(shape, 1) // HEAD) == head


def block_ones(size):
    shape = (size, size)
    return jnp.where(iota(shape, 0) // HEAD == iota(shape, 1) // HEAD, 1.0, 0.0).astype(BF16)


def group_sum(value, ones):
    high, low = halves(value)
    return mm(high, ones) + mm(low, ones)


def expand(compact):
    shape = (LANES, LANES)
    tall = jnp.concatenate([compact] * (LANES // HEAD), axis=0)
    return jnp.where(iota(shape, 0) // HEAD == iota(shape, 1) // HEAD, tall, 0.0)


def shrink(full):
    parts = [full[HEAD * h : HEAD * (h + 1)] for h in range(LANES // HEAD)]
    return (parts[0] + parts[1]) + (parts[2] + parts[3])


def unit_state():
    shape = (HEAD, LANES)
    eye = jnp.where(iota(shape, 0) == iota(shape, 1) % HEAD, 1.0, 0.0)
    return jnp.concatenate([eye, jnp.zeros(shape, F32)], axis=0)


def follow(earlier, trans, base):
    moved = mm3(earlier, expand(trans))
    return jnp.concatenate([moved[:HEAD], moved[HEAD:] + base], axis=0)


def per_chunk(rows):
    return jnp.concatenate([jnp.broadcast_to(row, (SPAN, LANES)) for row in rows], axis=0)


def swap_pair(value):
    return pltpu.roll(value, HEAD, 1)


def local_kernel(*refs):
    sources = refs[:14]
    pack_out, prior_out, conv_out, normed, fall_out, start_out = refs[14:20]
    erase_out, key_out, value_out, weave_out, removed_out = refs[20:25]
    late_weights = refs[25:27]
    tokens, gain, key_gain, bias, shift, extra = refs[27:33]
    weights = refs[33:37]
    conv_weights = refs[37]
    sems = refs[38]
    targets = (
        tokens,
        gain,
        key_gain,
        bias,
        shift,
        extra,
        *weights,
        conv_weights.at[:, :CONV],
        conv_weights.at[:, CONV:],
        *late_weights,
    )
    copies = [
        pltpu.make_async_copy(source, target, sems.at[n])
        for n, (source, target) in enumerate(zip(sources, targets))
    ]
    for n in (0, 1, 6, 2, 7, 8, 3, 4, 5, 9, 10, 11, 12, 13):
        copies[n].start()
    copies[0].wait()
    copies[1].wait()
    for n in range(ROWS // 16):
        here = slice(16 * n, 16 * n + 16)
        rows = tokens[here].astype(F32)
        scale = lax.rsqrt(jnp.mean(rows * rows, axis=-1, keepdims=True) + NORM_EPS)
        normed[here] = (rows * scale * gain[...]).astype(BF16)

    def project(n):
        copies[n].wait()
        return rounded_product(normed[...], targets[n][...])

    square = (ROWS, LANES)
    row_at, lane_at = iota(square, 0), iota(square, 1)
    ones = block_ones(LANES)

    key = project(6)
    copies[2].wait()
    key_scaled = key * key_gain[...]
    unit = key_scaled * lax.rsqrt(group_sum(key_scaled * key_scaled, ones) + KEY_EPS)
    erase = unit * jax.nn.sigmoid(project(7))
    decay = project(8)
    for n in (3, 4, 5):
        copies[n].wait()
    logits = decay + bias[...] + shift[...]
    log_decay = extra[...] - EXP_HALF * jax.nn.sigmoid(logits)
    small = (SPAN, SPAN)
    lower = jnp.where(iota(small, 1) <= iota(small, 0), 1.0, 0.0).astype(BF16)
    part_high, part_mid = halves(log_decay)
    part_low = (log_decay - part_high.astype(F32) - part_mid.astype(F32)).astype(BF16)
    chunks = [slice(SPAN * c, SPAN * c + SPAN) for c in range(CHUNKS)]
    cumulate = jnp.concatenate(
        [
            mm(lower, part_high[at]) + (mm(lower, part_mid[at]) + mm(lower, part_low[at]))
            for at in chunks
        ],
        axis=0,
    )
    before = cumulate - log_decay
    mids = [cumulate[SPAN * c + 31 : SPAN * c + 32] for c in range(CHUNKS)]
    finals = [cumulate[SPAN * c + 63 : SPAN * c + 64] for c in range(CHUNKS)]
    mid = per_chunk(mids)
    rise = jnp.exp(mid - cumulate)
    fall_out[...] = jnp.exp(cumulate - mid)
    unit_s = unit * jnp.exp(before - mid)
    erase_s = erase * rise
    key_s = key * rise
    starts = [jnp.exp(m) for m in mids]
    for c in range(CHUNKS):
        start_out[c : c + 1] = starts[c]
    to_end = per_chunk([jnp.exp(f - m) for f, m in zip(finals, mids)])
    unit_q = unit_s * per_chunk(starts)
    kept_erase = (erase_s * to_end).astype(BF16)
    kept_key = (key_s * to_end).astype(BF16)
    erase_b = erase_s.astype(BF16)
    key_b = key_s.astype(BF16)
    unit_b = unit_s.astype(BF16)
    value_b = project(9).astype(BF16)
    erase_out[...] = erase_b
    key_out[...] = key_b
    value_out[...] = value_b

    copies[10].wait()
    copies[11].wait()
    both = rounded_product(normed[...], conv_weights[...])
    conv_input = rounded(both[:, :CONV] * jax.nn.sigmoid(both[:, CONV:]))
    conv_out[...] = conv_input
    pack_out[2 * HEAD :, :128] = conv_input[ROWS - 32 : ROWS - 16]
    pack_out[2 * HEAD :, 128:] = conv_input[ROWS - 16 :]

    flat = (SPAN, LANES)
    row_in, lane_in = iota(flat, 0), iota(flat, 1) % HEAD
    strict = lane_in < row_in
    near = strict & (row_in // 8 == lane_in // 8)
    far = strict & (row_in // 8 != lane_in // 8)

    def spread(value):
        return jnp.concatenate([value.astype(BF16)] * 4, axis=0) * ones

    def times(left, right):
        return [mm(x, spread(y)) for x, y in zip(left, right)]

    def add(*terms):
        return [functools.reduce(lambda p, q: p + q, group) for group in zip(*terms)]

    erase_mix = [mm(unit_b[at], spread(erase_b[at]), NT) for at in chunks]
    key_mix = [
        jnp.where(strict, mm(unit_b[at], spread(key_b[at]), NT), 0.0) for at in chunks
    ]
    d1 = [jnp.where(near, a, 0.0) for a in erase_mix]
    n1 = [jnp.where(far, a, 0.0) for a in erase_mix]
    d2 = times(d1, d1)
    key_value = times(key_mix, [value_b[at] for at in chunks])
    stacked = times([jnp.concatenate([p, q], axis=0) for p, q in zip(d1, d2)], d2)
    d4 = [m[SPAN:] for m in stacked]
    g = [q - p - m[:SPAN] for p, q, m in zip(d1, d2, stacked)]
    dinv = add(g, d4, times(g, d4))
    p1 = add(n1, times(dinv, n1))
    p2 = times(p1, p1)
    m1 = [d - p - r for d, p, r in zip(dinv, p1, times(p1, dinv))]
    p4 = times(p2, p2)
    m2 = add(m1, p2, times(p2, m1))
    m3 = add(m2, p4, times(p4, m2))
    start_unit = [unit_q[at] for at in chunks]
    weave = [-x for x in add(start_unit, times(m3, start_unit))]
    removed = [-x for x in add(key_value, times(m3, key_value))]
    weave = [x.astype(BF16) for x in weave]
    removed = [x.astype(BF16) for x in removed]

    same_head = row_at // HEAD == lane_at // HEAD
    eye = row_at == lane_at
    state = unit_state()
    for c, at in enumerate(chunks):
        weave_out[at] = weave[c]
        removed_out[at] = removed[c]
        prior_out[c] = state
        trans = jnp.where(same_head, mm(weave[c], kept_erase[at], TN), 0.0) + jnp.where(
            eye, jnp.broadcast_to(jnp.exp(finals[c]), square), 0.0
        )
        base = mm(
            jnp.concatenate([removed[c], value_b[at]], axis=0),
            jnp.concatenate([kept_erase[at], kept_key[at]], axis=0),
            TN,
        )
        base = shrink(jnp.where(same_head, base, 0.0))
        if c == 0:
            state = jnp.concatenate([shrink(trans), base], axis=0)
        else:
            moved = mm3(state, trans)
            state = jnp.concatenate([moved[:HEAD], moved[HEAD:] + base], axis=0)
    pack_out[: 2 * HEAD] = state
    copies[12].wait()
    copies[13].wait()


def rounded(value):
    return value.astype(BF16).astype(F32)


def rounded_product(left, right):
    return rounded(jnp.dot(left, right, preferred_element_type=F32))


def gate_kernel(normed, w_receptance, w_gate, receptance_out, gate_out):
    receptance_out[...] = rounded_product(normed[...], w_receptance[...])
    gate_out[...] = jax.nn.sigmoid(rounded_product(normed[...], w_gate[...]))


def read_kernel(
    receptance,
    fall,
    start,
    erase,
    key,
    value,
    weave,
    removed,
    priors,
    local_out,
    query_out,
):
    ones = block_ones(LANES)
    flat = (SPAN, LANES)
    inclusive = iota(flat, 1) % HEAD <= iota(flat, 0)

    def spread(part):
        return jnp.concatenate([part.astype(BF16)] * 4, axis=0) * ones

    for c in range(CHUNKS):
        here = slice(SPAN * c, SPAN * c + SPAN)
        read_s = receptance[here] * fall[here]
        read_b = read_s.astype(BF16)
        read_erase = jnp.where(inclusive, mm(read_b, spread(erase[here]), NT), 0.0)
        read_key = jnp.where(inclusive, mm(read_b, spread(key[here]), NT), 0.0)
        query = read_s * start[c : c + 1] + mm(read_erase, spread(weave[here]))
        local = mm(read_erase, spread(removed[here])) + mm(read_key, spread(value[here]))
        if c:
            prior = priors[c]
            local = local + mm(query, spread(prior[HEAD:]), NT)
            query = mm(query, spread(prior[:HEAD]), NT)
        local_out[here] = local
        query_out[here] = query.astype(BF16)


def conv_kernel(conv_in, taps, gain, shift, done_out, part_out, padded):
    padded[:HALO] = jnp.zeros((HALO, CONV), F32)
    padded[HALO:] = conv_in[...]
    total = jnp.zeros((ROWS, CONV), F32)
    for j in range(TAPS):
        total = total + taps[j : j + 1] * padded[2 + j : 2 + j + ROWS]
    part_out[...] = total[:HALO]
    done_out[...] = finish_conv(total, gain[...], shift[...])


def finish_conv(total, gain, shift):
    ones = block_ones(CONV)
    centred = total - group_sum(total, ones) * (1.0 / HEAD)
    spread = group_sum(centred * centred, ones) * (1.0 / HEAD)
    scaled = centred * lax.rsqrt(spread + GROUP_EPS) * gain + shift
    return (scaled * jax.nn.sigmoid(scaled)).astype(BF16)


def joined(lower, upper):
    return follow(lower[: 2 * HEAD], upper[:HEAD], upper[HEAD : 2 * HEAD])


def core_kernel(mine, other, pack_out, prefix_out, total_out):
    first = lax.axis_index("c") == 0
    early = jnp.where(first, mine[...], other[...])
    late = jnp.where(first, other[...], mine[...])
    total = joined(early, late)
    total_out[...] = total
    pack_out[: 2 * HEAD] = total.astype(BF16)
    pack_out[2 * HEAD :] = late[2 * HEAD :].astype(BF16)
    prefix_out[: 2 * HEAD] = jnp.where(first, unit_state(), early[: 2 * HEAD])
    prefix_out[2 * HEAD :] = jnp.where(first, 0.0, early[2 * HEAD :])


def row_kernel(own, total, from_1, from_2, from_3, prefix, *refs):
    pack_out, prefix_out, slots = refs[-3:]
    me, core = lax.axis_index("y"), lax.axis_index("c")
    slots[0, : 2 * HEAD] = total[...]
    slots[0, 2 * HEAD :] = own[2 * HEAD :].astype(F32)
    for n, ref in enumerate((from_1, from_2, from_3)):
        slots[n + 1] = ref[...].astype(F32)
    state = slots[me ^ 0][: 2 * HEAD]
    before = unit_state()
    for n in range(1, 4):
        before = jnp.where(me == n, state, before)
        piece = slots[me ^ n]
        state = follow(state, piece[:HEAD], piece[HEAD : 2 * HEAD])
    pack_out[: 2 * HEAD] = state.astype(BF16)
    pack_out[2 * HEAD :] = slots[me ^ 3, 2 * HEAD :].astype(BF16)
    prefix_out[: 2 * HEAD] = follow(before, prefix[:HEAD], prefix[HEAD : 2 * HEAD])
    behind = slots[me ^ jnp.maximum(me - 1, 0), 2 * HEAD :]
    takes = (me > 0) & (core == 0)
    prefix_out[2 * HEAD :] = jnp.where(takes, behind, prefix[2 * HEAD :])


def last_kernel(
    from_1,
    from_2,
    from_3,
    prefix,
    local,
    query,
    gate,
    head_gain,
    conv_done,
    conv_part,
    taps,
    conv_gain,
    conv_shift,
    out_0,
    out_1,
    out_2,
    out_3,
    slots,
    ready,
    padded,
):
    z, y, c, x = (lax.axis_index(name) for name in SP_TP)
    for n, ref in enumerate((from_1, from_2, from_3)):
        slots[n + 1] = ref[...].astype(F32)
    slots[0] = slots[1]
    state = jnp.where(z > 0, slots[z ^ 0, HEAD : 2 * HEAD], 0.0)
    for n in range(1, 3):
        piece = slots[z ^ n]
        moved = mm3(state, expand(piece[:HEAD])) + piece[HEAD : 2 * HEAD]
        state = jnp.where(n < z, moved, state)
    state = mm3(state, expand(prefix[:HEAD])) + prefix[HEAD : 2 * HEAD]
    readout = local[...] + mm(query[...], expand(state), NT)
    ones = block_ones(LANES)
    centred = readout - group_sum(readout, ones) * (1.0 / HEAD)
    spread = group_sum(centred * centred, ones) * (1.0 / HEAD)
    mixed = centred * lax.rsqrt(spread + HEAD_EPS) * head_gain[...] * gate[...]
    ready[:, CONV:] = mixed.astype(BF16)
    ready[:, :CONV] = conv_done[...]

    behind = slots[z ^ jnp.maximum(z - 1, 0), 2 * HEAD :]
    takes = (z > 0) & (y == 0) & (c == 0)
    side = jnp.where(takes, behind, prefix[2 * HEAD :])
    padded[:16] = side[:, :128]
    padded[16:32] = side[:, 128:]
    padded[32:] = jnp.zeros((HALO, CONV), F32)
    total = conv_part[...]
    for j in range(TAPS):
        total = total + taps[j : j + 1] * padded[2 + j : 2 + j + HALO]
    ready[:HALO, :CONV] = finish_conv(total, conv_gain[...], conv_shift[...])
    for n, out in enumerate((out_0, out_1, out_2, out_3)):
        to = x ^ n
        out[...] = ready[pl.ds(pl.multiple_of(to * SPAN, SPAN), SPAN)]


def project_kernel(own, from_1, from_2, from_3, conv_w, mix_w, out, conv_rows, mix_rows):
    x = lax.axis_index("x")
    for n, ref in enumerate((own, from_1, from_2, from_3)):
        of = x ^ n
        conv_rows[:, pl.ds(pl.multiple_of(of * CONV, CONV), CONV)] = ref[:, :CONV]
        mix_rows[:, pl.ds(pl.multiple_of(of * LANES, LANES), LANES)] = ref[:, CONV:]
    total = jnp.dot(conv_rows[...], conv_w[...], preferred_element_type=F32)
    total = total + jnp.dot(mix_rows[...], mix_w[...], preferred_element_type=F32)
    out[...] = total.astype(BF16)


def swapped(value, axes, bits):
    count = lax.axis_size(axes)
    return lax.ppermute(value, axes, [(s, s ^ bits) for s in range(count)])


def params():
    return pltpu.CompilerParams(vmem_limit_bytes=40 * 1024 * 1024)


def call(kernel, name, outs, arguments, specs=None, scratch=(), pinned=False):
    if pinned:
        arguments = [pltpu.with_memory_space_constraint(a, pltpu.HBM) for a in arguments]
    return pl.pallas_call(
        kernel,
        name=name,
        out_shape=[jax.ShapeDtypeStruct(*o) for o in outs],
        in_specs=specs or [VMEM] * len(arguments),
        out_specs=[VMEM] * len(outs),
        scratch_shapes=list(scratch),
        compiler_params=params(),
    )(*arguments)


def local(
    tokens,
    input_norm_gain,
    convolution_value_weight,
    convolution_gate_weight,
    depthwise_taps_weight,
    convolution_group_gain,
    convolution_group_shift,
    receptance_weight,
    key_weight,
    value_weight,
    decay_weight,
    correction_rate_weight,
    output_gate_weight,
    key_prenorm_gain,
    decay_offset_bias,
    position_decay_shift,
    extra_log_decay,
    head_norm_gain,
    convolution_output_weight,
    attention_output_weight,
):
    def as_row(value):
        return value.reshape(1, value.shape[0])

    conv_gain, conv_shift = as_row(convolution_group_gain), as_row(convolution_group_shift)
    wide = pltpu.VMEM((2048, LANES), BF16)
    row = pltpu.VMEM((1, LANES), F32)
    square = ((ROWS, LANES), F32)
    square_b = ((ROWS, LANES), BF16)
    state = ((2 * HEAD, LANES), F32)
    packed = ((PACK, LANES), F32)
    packed_b = ((PACK, LANES), BF16)
    (
        pack,
        priors,
        conv_input,
        normed,
        fall,
        start,
        erase,
        key,
        value,
        weave,
        removed,
        w_receptance,
        w_gate,
    ) = call(
        local_kernel,
        "local",
        [
            packed,
            ((CHUNKS, 2 * HEAD, LANES), F32),
            ((ROWS, CONV), F32),
            ((ROWS, 2048), BF16),
            square,
            ((8, LANES), F32),
        ]
        + [square_b] * 5
        + [((2048, LANES), BF16)] * 2,
        (
            tokens,
            as_row(input_norm_gain),
            as_row(key_prenorm_gain),
            as_row(decay_offset_bias),
            position_decay_shift,
            extra_log_decay,
            key_weight,
            correction_rate_weight,
            decay_weight,
            value_weight,
            convolution_value_weight,
            convolution_gate_weight,
            receptance_weight,
            output_gate_weight,
        ),
        specs=[HBM] * 14,
        pinned=True,
        scratch=[pltpu.VMEM((ROWS, 2048), BF16), pltpu.VMEM((1, 2048), F32), row, row]
        + [pltpu.VMEM((ROWS, LANES), F32)] * 2
        + [wide] * 5
        + [pltpu.SemaphoreType.DMA((14,))],
    )
    other = swapped(pack, "c", 1)
    pack, prefix, total = call(core_kernel, "core", [packed_b, packed, state], (pack, other))
    receptance, gate = call(
        gate_kernel,
        "gate",
        [square, square],
        (normed, w_receptance, w_gate),
    )
    local_read, query = call(
        read_kernel,
        "read",
        [square, square_b],
        (receptance, fall, start, erase, key, value, weave, removed, priors),
    )
    conv_done, conv_part = call(
        conv_kernel,
        "conv",
        [((ROWS, CONV), BF16), ((HALO, CONV), F32)],
        (conv_input, depthwise_taps_weight, conv_gain, conv_shift),
        scratch=[pltpu.VMEM((HALO + ROWS, CONV), F32)],
    )
    planes = [swapped(pack, ("y", "c"), 2 * n + 1) for n in (1, 2, 3)]
    pack, prefix = call(
        row_kernel,
        "row",
        [packed_b, packed],
        (pack, total, *planes, prefix, conv_done, gate),
        specs=[VMEM] * 6 + [ANY] * 2,
        scratch=[pltpu.VMEM((4, PACK, LANES), F32)],
    )
    planes = [swapped(pack, ("z", "c"), 2 * n + 1) for n in (1, 2, 3)]
    sends = call(
        last_kernel,
        "last",
        [((SPAN, CONV + LANES), BF16)] * 4,
        (
            *planes,
            prefix,
            local_read,
            query,
            gate,
            as_row(head_norm_gain),
            conv_done,
            conv_part,
            depthwise_taps_weight,
            conv_gain,
            conv_shift,
        ),
        scratch=[
            pltpu.VMEM((4, PACK, LANES), F32),
            pltpu.VMEM((ROWS, CONV + LANES), BF16),
            pltpu.VMEM((2 * HALO, CONV), F32),
        ],
    )
    arrived = [swapped(sends[n], "x", n) for n in (1, 2, 3)]
    (mixed,) = call(
        project_kernel,
        "project",
        [((SPAN, 2048), BF16)],
        (sends[0], *arrived, convolution_output_weight, attention_output_weight),
        scratch=[pltpu.VMEM((SPAN, 512), BF16), pltpu.VMEM((SPAN, 1024), BF16)],
    )
    return mixed


def solution(mesh):
    split = Mesh(mesh.devices.reshape(4, 4, 2, mesh.shape["tp"]), SP_TP)
    placed = (
        P(SP, None),
        P(),
        P(None, "x"),
        P(None, "x"),
        P(None, "x"),
        P("x"),
        P("x"),
        P(None, "x"),
        P(None, "x"),
        P(None, "x"),
        P(None, "x"),
        P(None, "x"),
        P(None, "x"),
        P("x"),
        P("x"),
        P(SP, "x"),
        P(SP, "x"),
        P("x"),
        P(),
        P(),
    )
    return jax.shard_map(
        local, mesh=split, in_specs=placed, out_specs=P(SP_TP, None), check_vma=False
    )
```

```python
import functools

import jax
import jax.numpy as jnp
from jax import lax
from jax.experimental import pallas as pl
from jax.experimental.pallas import tpu as pltpu
from jax.sharding import Mesh
from jax.sharding import PartitionSpec as P

HEAD = 64
ROWS = 256
LANES = 256
CONV = 128
SPAN = 64
CHUNKS = ROWS // SPAN
HALO = 32
TAPS = 31
PACK = 2 * HEAD + HALO // 2
SP = ("z", "y", "c")
SP_TP = ("z", "y", "c", "x")

NORM_EPS = 1e-06
GROUP_EPS = 1e-05
HEAD_EPS = 0.00064
KEY_EPS = 1e-06
EXP_HALF = 0.6065306597126334

F32 = jnp.float32
BF16 = jnp.bfloat16
NN = (((1,), (0,)), ((), ()))
NT = (((1,), (1,)), ((), ()))
TN = (((0,), (0,)), ((), ()))
VMEM = pl.BlockSpec(memory_space=pltpu.VMEM)
HBM = pl.BlockSpec(memory_space=pltpu.HBM)
ANY = pl.BlockSpec(memory_space=pl.ANY)


def mm(left, right, dims=NN):
    return lax.dot_general(
        left.astype(BF16), right.astype(BF16), dims, preferred_element_type=F32
    )


def halves(value):
    high = value.astype(BF16)
    return high, (value - high.astype(F32)).astype(BF16)


def mm3(left, right, dims=NN):
    left_high, left_low = halves(left)
    right_high, right_low = halves(right)
    return mm(left_high, right_high, dims) + (
        mm(left_high, right_low, dims) + mm(left_low, right_high, dims)
    )


def iota(shape, dim):
    return lax.broadcasted_iota(jnp.int32, shape, dim)


def head_lanes(shape, head):
    return (iota(shape, 1) // HEAD) == head


def block_ones(size):
    shape = (size, size)
    return jnp.where(iota(shape, 0) // HEAD == iota(shape, 1) // HEAD, 1.0, 0.0).astype(BF16)


def group_sum(value, ones):
    high, low = halves(value)
    return mm(high, ones) + mm(low, ones)


def expand(compact):
    shape = (LANES, LANES)
    tall = jnp.concatenate([compact] * (LANES // HEAD), axis=0)
    return jnp.where(iota(shape, 0) // HEAD == iota(shape, 1) // HEAD, tall, 0.0)


def shrink(full):
    parts = [full[HEAD * h : HEAD * (h + 1)] for h in range(LANES // HEAD)]
    return (parts[0] + parts[1]) + (parts[2] + parts[3])


def unit_state():
    shape = (HEAD, LANES)
    eye = jnp.where(iota(shape, 0) == iota(shape, 1) % HEAD, 1.0, 0.0)
    return jnp.concatenate([eye, jnp.zeros(shape, F32)], axis=0)


def follow(earlier, trans, base):
    moved = mm3(earlier, expand(trans))
    return jnp.concatenate([moved[:HEAD], moved[HEAD:] + base], axis=0)


def per_chunk(rows):
    return jnp.concatenate([jnp.broadcast_to(row, (SPAN, LANES)) for row in rows], axis=0)


def swap_pair(value):
    return pltpu.roll(value, HEAD, 1)


def local_kernel(*refs):
    sources = refs[:14]
    pack_out, prior_out, conv_out, normed, fall_out, start_out = refs[14:20]
    erase_out, key_out, value_out, weave_out, removed_out = refs[20:25]
    late_weights = refs[25:27]
    tokens, gain, key_gain, bias, shift, extra = refs[27:33]
    weights = refs[33:37]
    conv_weights = refs[37]
    sems = refs[38]
    targets = (
        tokens,
        gain,
        key_gain,
        bias,
        shift,
        extra,
        *weights,
        conv_weights.at[:, :CONV],
        conv_weights.at[:, CONV:],
        *late_weights,
    )
    copies = [
        pltpu.make_async_copy(source, target, sems.at[n])
        for n, (source, target) in enumerate(zip(sources, targets))
    ]
    blocks = (0, 14, 15, 16)
    parts = [slice(SPAN * n, SPAN * n + SPAN) for n in range(CHUNKS)]
    copies[0] = pltpu.make_async_copy(sources[0].at[parts[0]], tokens.at[parts[0]], sems.at[0])
    for n in range(1, CHUNKS):
        copies.append(
            pltpu.make_async_copy(sources[0].at[parts[n]], tokens.at[parts[n]], sems.at[13 + n])
        )

    def start(*which):
        for n in which:
            copies[n].start()

    start(*blocks, 1, 6, 2, 7)
    copies[1].wait()
    for n in range(CHUNKS):
        copies[blocks[n]].wait()
        if n == 0:
            start(8)
        for m in range(SPAN // 16):
            here = slice(SPAN * n + 16 * m, SPAN * n + 16 * m + 16)
            rows = tokens[here].astype(F32)
            scale = lax.rsqrt(jnp.mean(rows * rows, axis=-1, keepdims=True) + NORM_EPS)
            normed[here] = (rows * scale * gain[...]).astype(BF16)
    start(3, 4, 5, 9)

    def project(n):
        copies[n].wait()
        return rounded_product(normed[...], targets[n][...])

    square = (ROWS, LANES)
    row_at, lane_at = iota(square, 0), iota(square, 1)
    ones = block_ones(LANES)

    key = project(6)
    copies[2].wait()
    key_scaled = key * key_gain[...]
    unit = key_scaled * lax.rsqrt(group_sum(key_scaled * key_scaled, ones) + KEY_EPS)
    erase = unit * jax.nn.sigmoid(project(7))
    start(10, 11)
    decay = project(8)
    start(12, 13)
    for n in (3, 4, 5):
        copies[n].wait()
    logits = decay + bias[...] + shift[...]
    log_decay = extra[...] - EXP_HALF * jax.nn.sigmoid(logits)
    small = (SPAN, SPAN)
    lower = jnp.where(iota(small, 1) <= iota(small, 0), 1.0, 0.0).astype(BF16)
    part_high, part_mid = halves(log_decay)
    part_low = (log_decay - part_high.astype(F32) - part_mid.astype(F32)).astype(BF16)
    chunks = [slice(SPAN * c, SPAN * c + SPAN) for c in range(CHUNKS)]
    cumulate = jnp.concatenate(
        [
            mm(lower, part_high[at]) + (mm(lower, part_mid[at]) + mm(lower, part_low[at]))
            for at in chunks
        ],
        axis=0,
    )
    before = cumulate - log_decay
    mids = [cumulate[SPAN * c + 31 : SPAN * c + 32] for c in range(CHUNKS)]
    finals = [cumulate[SPAN * c + 63 : SPAN * c + 64] for c in range(CHUNKS)]
    mid = per_chunk(mids)
    rise = jnp.exp(mid - cumulate)
    fall_out[...] = jnp.exp(cumulate - mid)
    unit_s = unit * jnp.exp(before - mid)
    erase_s = erase * rise
    key_s = key * rise
    starts = [jnp.exp(m) for m in mids]
    for c in range(CHUNKS):
        start_out[c : c + 1] = starts[c]
    to_end = per_chunk([jnp.exp(f - m) for f, m in zip(finals, mids)])
    unit_q = unit_s * per_chunk(starts)
    kept_erase = (erase_s * to_end).astype(BF16)
    kept_key = (key_s * to_end).astype(BF16)
    erase_b = erase_s.astype(BF16)
    key_b = key_s.astype(BF16)
    unit_b = unit_s.astype(BF16)
    erase_out[...] = erase_b
    key_out[...] = key_b
    flat = (SPAN, LANES)
    row_in, lane_in = iota(flat, 0), iota(flat, 1) % HEAD
    strict = lane_in < row_in
    near = strict & (row_in // 8 == lane_in // 8)
    far = strict & (row_in // 8 != lane_in // 8)

    def spread(value):
        return jnp.concatenate([value.astype(BF16)] * 4, axis=0) * ones

    def times(left, right):
        return [mm(x, spread(y)) for x, y in zip(left, right)]

    def add(*terms):
        return [functools.reduce(lambda p, q: p + q, group) for group in zip(*terms)]

    erase_mix = [mm(unit_b[at], spread(erase_b[at]), NT) for at in chunks]
    key_mix = [
        jnp.where(strict, mm(unit_b[at], spread(key_b[at]), NT), 0.0) for at in chunks
    ]
    d1 = [jnp.where(near, a, 0.0) for a in erase_mix]
    n1 = [jnp.where(far, a, 0.0) for a in erase_mix]
    d2 = times(d1, d1)
    stacked = times([jnp.concatenate([p, q], axis=0) for p, q in zip(d1, d2)], d2)
    d4 = [m[SPAN:] for m in stacked]
    g = [q - p - m[:SPAN] for p, q, m in zip(d1, d2, stacked)]
    dinv = add(g, d4, times(g, d4))
    p1 = add(n1, times(dinv, n1))
    p2 = times(p1, p1)
    m1 = [d - p - r for d, p, r in zip(dinv, p1, times(p1, dinv))]
    p4 = times(p2, p2)
    m2 = add(m1, p2, times(p2, m1))
    m3 = add(m2, p4, times(p4, m2))
    value_b = project(9).astype(BF16)
    value_out[...] = value_b
    key_value = times(key_mix, [value_b[at] for at in chunks])
    start_unit = [unit_q[at] for at in chunks]
    weave = [-x for x in add(start_unit, times(m3, start_unit))]
    removed = [-x for x in add(key_value, times(m3, key_value))]
    weave = [x.astype(BF16) for x in weave]
    removed = [x.astype(BF16) for x in removed]

    copies[10].wait()
    copies[11].wait()
    both = rounded_product(normed[...], conv_weights[...])
    conv_input = rounded(both[:, :CONV] * jax.nn.sigmoid(both[:, CONV:]))
    conv_out[...] = conv_input
    pack_out[2 * HEAD :, :128] = conv_input[ROWS - 32 : ROWS - 16]
    pack_out[2 * HEAD :, 128:] = conv_input[ROWS - 16 :]

    same_head = row_at // HEAD == lane_at // HEAD
    eye = row_at == lane_at
    state = unit_state()
    for c, at in enumerate(chunks):
        weave_out[at] = weave[c]
        removed_out[at] = removed[c]
        prior_out[c] = state
        trans = jnp.where(same_head, mm(weave[c], kept_erase[at], TN), 0.0) + jnp.where(
            eye, jnp.broadcast_to(jnp.exp(finals[c]), square), 0.0
        )
        base = mm(
            jnp.concatenate([removed[c], value_b[at]], axis=0),
            jnp.concatenate([kept_erase[at], kept_key[at]], axis=0),
            TN,
        )
        base = shrink(jnp.where(same_head, base, 0.0))
        if c == 0:
            state = jnp.concatenate([shrink(trans), base], axis=0)
        else:
            moved = mm3(state, trans)
            state = jnp.concatenate([moved[:HEAD], moved[HEAD:] + base], axis=0)
    pack_out[: 2 * HEAD] = state
    copies[12].wait()
    copies[13].wait()


def rounded(value):
    return value.astype(BF16).astype(F32)


def rounded_product(left, right):
    return rounded(jnp.dot(left, right, preferred_element_type=F32))


def gate_kernel(normed, w_receptance, w_gate, receptance_out, gate_out):
    receptance_out[...] = rounded_product(normed[...], w_receptance[...])
    gate_out[...] = jax.nn.sigmoid(rounded_product(normed[...], w_gate[...]))


def read_kernel(
    receptance,
    fall,
    start,
    erase,
    key,
    value,
    weave,
    removed,
    priors,
    local_out,
    query_out,
):
    ones = block_ones(LANES)
    flat = (SPAN, LANES)
    inclusive = iota(flat, 1) % HEAD <= iota(flat, 0)

    def spread(part):
        return jnp.concatenate([part.astype(BF16)] * 4, axis=0) * ones

    for c in range(CHUNKS):
        here = slice(SPAN * c, SPAN * c + SPAN)
        read_s = receptance[here] * fall[here]
        read_b = read_s.astype(BF16)
        read_erase = jnp.where(inclusive, mm(read_b, spread(erase[here]), NT), 0.0)
        read_key = jnp.where(inclusive, mm(read_b, spread(key[here]), NT), 0.0)
        query = read_s * start[c : c + 1] + mm(read_erase, spread(weave[here]))
        local = mm(read_erase, spread(removed[here])) + mm(read_key, spread(value[here]))
        if c:
            prior = priors[c]
            local = local + mm(query, spread(prior[HEAD:]), NT)
            query = mm(query, spread(prior[:HEAD]), NT)
        local_out[here] = local
        query_out[here] = query.astype(BF16)


def conv_kernel(conv_in, taps, gain, shift, done_out, part_out, padded):
    padded[:HALO] = jnp.zeros((HALO, CONV), F32)
    padded[HALO:] = conv_in[...]
    total = jnp.zeros((ROWS, CONV), F32)
    for j in range(TAPS):
        total = total + taps[j : j + 1] * padded[2 + j : 2 + j + ROWS]
    part_out[...] = total[:HALO]
    done_out[...] = finish_conv(total, gain[...], shift[...])


def finish_conv(total, gain, shift):
    ones = block_ones(CONV)
    centred = total - group_sum(total, ones) * (1.0 / HEAD)
    spread = group_sum(centred * centred, ones) * (1.0 / HEAD)
    scaled = centred * lax.rsqrt(spread + GROUP_EPS) * gain + shift
    return (scaled * jax.nn.sigmoid(scaled)).astype(BF16)


def joined(lower, upper):
    return follow(lower[: 2 * HEAD], upper[:HEAD], upper[HEAD : 2 * HEAD])


def core_kernel(mine, other, pack_out, prefix_out, total_out):
    first = lax.axis_index("c") == 0
    early = jnp.where(first, mine[...], other[...])
    late = jnp.where(first, other[...], mine[...])
    total = joined(early, late)
    total_out[...] = total
    pack_out[: 2 * HEAD] = total.astype(BF16)
    pack_out[2 * HEAD :] = late[2 * HEAD :].astype(BF16)
    prefix_out[: 2 * HEAD] = jnp.where(first, unit_state(), early[: 2 * HEAD])
    prefix_out[2 * HEAD :] = jnp.where(first, 0.0, early[2 * HEAD :])


def in_order(own, total, pieces, slots):
    me = lax.axis_index("y")
    slots[0, : 2 * HEAD] = total[...]
    slots[0, 2 * HEAD :] = own[2 * HEAD :].astype(F32)
    for n, ref in enumerate(pieces):
        slots[n + 1] = ref[...].astype(F32)
    return me


def row_kernel(own, total, from_3, from_2, from_1, _, unread, pack_out, total_out, slots):
    me = in_order(own, total, (from_1, from_2, from_3), slots)
    low = joined(slots[me], slots[me ^ 1])
    high = joined(slots[me ^ 2], slots[me ^ 3])
    state = joined(low, high)
    total_out[...] = state
    pack_out[: 2 * HEAD] = state.astype(BF16)
    pack_out[2 * HEAD :] = slots[me ^ 3, 2 * HEAD :].astype(BF16)


def prefix_kernel(own, total, from_3, from_2, from_1, prefix, prefix_out, slots):
    me = in_order(own, total, (from_1, from_2, from_3), slots)
    first = slots[me][: 2 * HEAD]
    two = joined(first, slots[me ^ 1])
    three = joined(two, slots[me ^ 2])
    before = jnp.where(me == 1, first, unit_state())
    before = jnp.where(me == 2, two, before)
    before = jnp.where(me == 3, three, before)
    prefix_out[: 2 * HEAD] = joined(before, prefix[...])
    behind = slots[me ^ jnp.maximum(me - 1, 0), 2 * HEAD :]
    takes = (me > 0) & (lax.axis_index("c") == 0)
    prefix_out[2 * HEAD :] = jnp.where(takes, behind, prefix[2 * HEAD :])


def plane_kernel(mine, total, other, prefix, pack_out, prefix_out):
    at = lax.axis_index("z")
    upper = lax.rem(at, 2) == 1
    got = other[...].astype(F32)
    states = got[: 2 * HEAD]
    early = jnp.where(upper, states, total[...])
    late = jnp.where(upper, total[...], states)
    base = mm3(early[HEAD:], expand(late[:HEAD])) + late[HEAD:]
    pack_out[:HEAD] = base.astype(BF16)
    pack_out[HEAD:] = jnp.where(upper, mine[2 * HEAD :].astype(F32), got[2 * HEAD :]).astype(BF16)
    behind = joined(states, prefix[...])
    prefix_out[: 2 * HEAD] = jnp.where(upper, behind, prefix[: 2 * HEAD])
    takes = upper & (lax.axis_index("c") == 0) & (lax.axis_index("y") == 0)
    prefix_out[2 * HEAD :] = jnp.where(takes, got[2 * HEAD :], prefix[2 * HEAD :])


def last_kernel(
    other,
    prefix,
    local,
    query,
    gate,
    head_gain,
    conv_done,
    conv_part,
    taps,
    conv_gain,
    conv_shift,
    out_0,
    out_1,
    out_2,
    out_3,
    ready,
    padded,
):
    z, y, c, x = (lax.axis_index(name) for name in SP_TP)
    got = other[...].astype(F32)
    entering = jnp.where(z >= 2, got[:HEAD], 0.0)
    state = mm3(entering, expand(prefix[:HEAD])) + prefix[HEAD : 2 * HEAD]
    readout = local[...] + mm(query[...], expand(state), NT)
    ones = block_ones(LANES)
    centred = readout - group_sum(readout, ones) * (1.0 / HEAD)
    spread = group_sum(centred * centred, ones) * (1.0 / HEAD)
    mixed = centred * lax.rsqrt(spread + HEAD_EPS) * head_gain[...] * gate[...]
    ready[:, CONV:] = mixed.astype(BF16)
    ready[:, :CONV] = conv_done[...]

    takes = (z >= 2) & (y == 0) & (c == 0) & (lax.rem(z, 2) == 0)
    side = jnp.where(takes, got[HEAD:], prefix[2 * HEAD :])
    padded[:16] = side[:, :128]
    padded[16:32] = side[:, 128:]
    padded[32:] = jnp.zeros((HALO, CONV), F32)
    total = conv_part[...]
    for j in range(TAPS):
        total = total + taps[j : j + 1] * padded[2 + j : 2 + j + HALO]
    ready[:HALO, :CONV] = finish_conv(total, conv_gain[...], conv_shift[...])
    for n, out in enumerate((out_0, out_1, out_2, out_3)):
        to = x ^ n
        out[...] = ready[pl.ds(pl.multiple_of(to * SPAN, SPAN), SPAN)]


def block_product(rows, of, conv_w, mix_w):
    conv = conv_w[pl.ds(pl.multiple_of(of * CONV, CONV), CONV)]
    mix = mix_w[pl.ds(pl.multiple_of(of * LANES, LANES), LANES)]
    return jnp.dot(rows[:, :CONV], conv, preferred_element_type=F32) + jnp.dot(
        rows[:, CONV:], mix, preferred_element_type=F32
    )


def part_kernel(partners, *refs):
    blocks = refs[: len(partners)]
    conv_w, mix_w, *sums, out = refs[len(partners) :]
    x = lax.axis_index("x")
    total = block_product(blocks[0], x ^ partners[0], conv_w, mix_w)
    for n, block in zip(partners[1:], blocks[1:]):
        total = total + block_product(block, x ^ n, conv_w, mix_w)
    for part in sums:
        total = total + part[...]
    out[...] = total.astype(out.dtype)


def swapped(value, axes, bits):
    count = lax.axis_size(axes)
    return lax.ppermute(value, axes, [(s, s ^ bits) for s in range(count)])


def params():
    return pltpu.CompilerParams(vmem_limit_bytes=40 * 1024 * 1024)


def call(kernel, name, outs, arguments, specs=None, scratch=(), pinned=False):
    if pinned:
        arguments = [pltpu.with_memory_space_constraint(a, pltpu.HBM) for a in arguments]
    return pl.pallas_call(
        kernel,
        name=name,
        out_shape=[jax.ShapeDtypeStruct(*o) for o in outs],
        in_specs=specs or [VMEM] * len(arguments),
        out_specs=[VMEM] * len(outs),
        scratch_shapes=list(scratch),
        compiler_params=params(),
    )(*arguments)


def local(
    tokens,
    input_norm_gain,
    convolution_value_weight,
    convolution_gate_weight,
    depthwise_taps_weight,
    convolution_group_gain,
    convolution_group_shift,
    receptance_weight,
    key_weight,
    value_weight,
    decay_weight,
    correction_rate_weight,
    output_gate_weight,
    key_prenorm_gain,
    decay_offset_bias,
    position_decay_shift,
    extra_log_decay,
    head_norm_gain,
    convolution_output_weight,
    attention_output_weight,
):
    def as_row(value):
        return value.reshape(1, value.shape[0])

    conv_gain, conv_shift = as_row(convolution_group_gain), as_row(convolution_group_shift)
    wide = pltpu.VMEM((2048, LANES), BF16)
    row = pltpu.VMEM((1, LANES), F32)
    square = ((ROWS, LANES), F32)
    square_b = ((ROWS, LANES), BF16)
    state = ((2 * HEAD, LANES), F32)
    packed = ((PACK, LANES), F32)
    packed_b = ((PACK, LANES), BF16)
    (
        pack,
        priors,
        conv_input,
        normed,
        fall,
        start,
        erase,
        key,
        value,
        weave,
        removed,
        w_receptance,
        w_gate,
    ) = call(
        local_kernel,
        "local",
        [
            packed,
            ((CHUNKS, 2 * HEAD, LANES), F32),
            ((ROWS, CONV), F32),
            ((ROWS, 2048), BF16),
            square,
            ((8, LANES), F32),
        ]
        + [square_b] * 5
        + [((2048, LANES), BF16)] * 2,
        (
            tokens,
            as_row(input_norm_gain),
            as_row(key_prenorm_gain),
            as_row(decay_offset_bias),
            position_decay_shift,
            extra_log_decay,
            key_weight,
            correction_rate_weight,
            decay_weight,
            value_weight,
            convolution_value_weight,
            convolution_gate_weight,
            receptance_weight,
            output_gate_weight,
        ),
        specs=[HBM] * 14,
        pinned=True,
        scratch=[pltpu.VMEM((ROWS, 2048), BF16), pltpu.VMEM((1, 2048), F32), row, row]
        + [pltpu.VMEM((ROWS, LANES), F32)] * 2
        + [wide] * 5
        + [pltpu.SemaphoreType.DMA((17,))],
    )
    other = swapped(pack, "c", 1)
    pack, prefix, total = call(core_kernel, "core", [packed_b, packed, state], (pack, other))
    receptance, gate = call(
        gate_kernel,
        "gate",
        [square, square],
        (normed, w_receptance, w_gate),
    )
    local_read, query = call(
        read_kernel,
        "read",
        [square, square_b],
        (receptance, fall, start, erase, key, value, weave, removed, priors),
    )
    conv_done, conv_part = call(
        conv_kernel,
        "conv",
        [((ROWS, CONV), BF16), ((HALO, CONV), F32)],
        (conv_input, depthwise_taps_weight, conv_gain, conv_shift),
        scratch=[pltpu.VMEM((HALO + ROWS, CONV), F32)],
    )
    planes = [swapped(pack, ("y", "c"), 2 * n + 1) for n in (3, 2, 1)]
    slots = pltpu.VMEM((4, PACK, LANES), F32)
    around = (pack, total, *planes)
    pack, total = call(
        row_kernel,
        "row",
        [packed_b, state],
        (*around, conv_done, gate),
        specs=[VMEM] * 5 + [ANY] * 2,
        scratch=[slots],
    )
    other = swapped(pack, ("z", "c"), 3)
    (prefix,) = call(prefix_kernel, "prefix", [packed], (*around, prefix), scratch=[slots])
    pack, prefix = call(
        plane_kernel,
        "plane",
        [((HEAD + HALO // 2, LANES), BF16), packed],
        (pack, total, other, prefix),
    )
    other = swapped(pack, ("z", "c"), 7)
    sends = call(
        last_kernel,
        "last",
        [((SPAN, CONV + LANES), BF16)] * 4,
        (
            other,
            prefix,
            local_read,
            query,
            gate,
            as_row(head_norm_gain),
            conv_done,
            conv_part,
            depthwise_taps_weight,
            conv_gain,
            conv_shift,
        ),
        scratch=[
            pltpu.VMEM((ROWS, CONV + LANES), BF16),
            pltpu.VMEM((2 * HALO, CONV), F32),
        ],
    )
    from_3, from_2, from_1 = [swapped(sends[n], "x", n) for n in (3, 2, 1)]
    weights = (convolution_output_weight, attention_output_weight)
    wide_sum = ((SPAN, 2048), F32)
    (own_sum,) = call(
        functools.partial(part_kernel, (0,)), "part_own", [wide_sum], (sends[0], *weights)
    )
    (near_sum,) = call(
        functools.partial(part_kernel, (3, 1)),
        "part_near",
        [wide_sum],
        (from_3, from_1, *weights, own_sum),
    )
    (mixed,) = call(
        functools.partial(part_kernel, (2,)),
        "part_far",
        [((SPAN, 2048), BF16)],
        (from_2, *weights, near_sum),
    )
    return mixed


def solution(mesh):
    split = Mesh(mesh.devices.reshape(4, 4, 2, mesh.shape["tp"]), SP_TP)
    placed = (
        P(SP, None),
        P(),
        P(None, "x"),
        P(None, "x"),
        P(None, "x"),
        P("x"),
        P("x"),
        P(None, "x"),
        P(None, "x"),
        P(None, "x"),
        P(None, "x"),
        P(None, "x"),
        P(None, "x"),
        P("x"),
        P("x"),
        P(SP, "x"),
        P(SP, "x"),
        P("x"),
        P(),
        P(),
    )
    return jax.shard_map(
        local, mesh=split, in_specs=placed, out_specs=P(SP_TP, None), check_vma=False
    )
```
